768 devices in a mesh: sp: 96 (over z, y), tp: 8 (over x, core).
Axes of the slice: x: 4, y: 8, z: 12, core: 2. Of those that a mesh axis runs over, the one named last changes fastest.
Arguments:
- queries: bfloat16 [1, 24576, 2048], P(None, 'sp', 'tp'), may hold values from -5 to 5
- key_vectors: bfloat16 [1, 24576, 2048], P(None, 'sp', 'tp'), may hold values from -5 to 5
- value_vectors: bfloat16 [1, 24576, 2048], P(None, 'sp', 'tp'), may hold values from -40 to 40
- cotangent: bfloat16 [1, 24576, 2048], P(None, 'sp', 'tp'), may hold values from -6 to 6
- out_gain: bfloat16 [2048], P('tp'), may hold values from 0.099609375 to 1.8984375
- rel_table: bfloat16 [16, 320], P('tp'), may hold values from -4 to 4
Outputs:
- grad_queries: bfloat16 [1, 24576, 2048], P(None, 'sp', 'tp')
- grad_keys: bfloat16 [1, 24576, 2048], P(None, 'sp', 'tp')
- grad_values: bfloat16 [1, 24576, 2048], P(None, 'sp', 'tp')
- grad_table: float32 [16, 320], P('tp')
The draws below stay inside these ranges and needn't reach their ends.
All inputs are finite; a program needn't handle non-finite values.
Results may differ from the reference program's by a relative error of at most 0.0071.
Values may be sent and summed in bfloat16 or wider, within the bound.
No kernel may reach another device: no remote copies, remote signals or barrier semaphores. Data moves between devices by JAX's collectives and lax.ppermute only.
A program may use at most 32 MiB of HBM per device.

```python
import math
import jax
import jax.numpy as jnp
import numpy as np
from jax import lax

HEADS = 16
HEAD_DIM = 128
SEG = 64
LEFT = 4
MAX_REL = 256
SEQS = 1
WIDTH = 2048
REL = 320
TOKENS = 24576


def head_scale():
    head_ids = (jnp.arange(WIDTH) // HEAD_DIM).astype(jnp.float32)
    return 3.0 ** (head_ids / (HEADS - 1))


def normal_rows(key, salt):
    normal_part = jax.random.normal(jax.random.fold_in(key, salt), (SEQS, TOKENS, WIDTH), jnp.float32)
    return jnp.clip(normal_part, -5.0, 5.0).reshape(SEQS, TOKENS // SEG, SEG, WIDTH)


def draw_queries(key, part):
    rows_out = normal_rows(key, 1)
    return rows_out.reshape(SEQS, TOKENS, WIDTH).astype(jnp.bfloat16)


def draw_key_vectors(key, part):
    rows_out = normal_rows(key, 2)
    return rows_out.reshape(SEQS, TOKENS, WIDTH).astype(jnp.bfloat16)


def draw_value_vectors(key, part):
    base_key = jax.random.fold_in(jax.random.fold_in(key, 3), 0)
    body_part = jnp.clip(jax.random.normal(base_key, (SEQS, TOKENS, WIDTH), jnp.float32), -4.0, 4.0)
    return (body_part * head_scale()).astype(jnp.bfloat16)


def block_levels(stream_key, extent, cuts, low, high):
    def one(position, blocks):
        draws = jax.random.uniform(jax.random.fold_in(jax.random.fold_in(stream_key, 6), position), (blocks,), jnp.float32, low / len(cuts), high / len(cuts))
        return jnp.repeat(jnp.exp(draws), extent[position] // blocks).reshape((-1,) + (1,) * (len(extent) - position - 1))

    factor_of = one(*cuts[0])
    for cut in cuts[1:]:
        factor_of = factor_of * one(*cut)
    return factor_of


def scatter_about(key, shape, spread, bound, shards=(), dtype=jnp.bfloat16):
    result = spread * jax.random.normal(key, shape, jnp.float32)
    if shards:
        result = result * block_levels(key, shape, shards, -0.22, 0.18)
    return jnp.clip(result, -bound, bound).astype(dtype)


def setup_inputs(seed: int = 0) -> dict:
    key_list = jax.random.split(jax.random.key(seed), 7)
    queries = draw_queries(jax.random.fold_in(key_list[6], 71), 0)
    key_vectors = draw_key_vectors(jax.random.fold_in(key_list[6], 71), 0)
    value_vectors = draw_value_vectors(jax.random.fold_in(key_list[6], 71), 0)
    cotangent = scatter_about(key_list[3], (SEQS, TOKENS, WIDTH), 1.0, 6.0, ((1, 96), (2, 8)))
    out_gain = jnp.clip(1.0 + 0.18 * jax.random.normal(key_list[4], (WIDTH,), jnp.float32), 0.099609375, 1.8984375).astype(jnp.bfloat16)
    rel_table = scatter_about(key_list[5], (HEADS, REL), 1.0, 4.0, ((0, 8),))
    return dict(queries=queries, key_vectors=key_vectors, value_vectors=value_vectors, cotangent=cotangent, out_gain=out_gain, rel_table=rel_table)


epsilon = 1e-06
masked_value = -1e+30

def band_index():
    query_pos = np.arange(SEG)[:, None, None]
    band_pos = np.arange(LEFT + 1)[None, :, None]
    key_pos = np.arange(SEG)[None, None, :]
    distance = (LEFT - band_pos) * SEG + query_pos - key_pos
    return (np.minimum(distance, MAX_REL) + SEG - 1).astype(np.int32)

def expand_bias(table_rows):
    return jnp.take(table_rows, jnp.asarray(band_index()), axis=1)

def padded_segments(rows_in):
    padded = jnp.pad(rows_in.astype(jnp.float32), ((LEFT * SEG, 0), (0, 0)))
    return padded.reshape(-1, SEG, HEAD_DIM)

def lowered(array):
    rounded = lax.optimization_barrier(array.astype(jnp.bfloat16))
    return rounded.astype(jnp.float32)

def head_probs(query_seg, key_pad, pos_bias, seg_count):
    scores = jnp.stack([jnp.einsum('cqd,ckd->cqk', query_seg, key_pad[offset:offset + seg_count]) for offset in range(LEFT + 1)], axis=2)
    scores = scores / math.sqrt(HEAD_DIM) + pos_bias[None]
    visible = np.arange(seg_count)[:, None] - LEFT + np.arange(LEFT + 1)[None, :] >= 0
    scores = jnp.where(visible[:, None, :, None], scores, masked_value)
    flat = jax.nn.softmax(scores.reshape(seg_count, SEG, -1), axis=-1)
    return flat.reshape(scores.shape)

def forward_head(packed):
    query_rows, key_rows, value_rows, pos_bias = packed
    seg_count = query_rows.shape[0] // SEG
    query_seg = query_rows.astype(jnp.float32).reshape(seg_count, SEG, HEAD_DIM)
    probability = head_probs(query_seg, padded_segments(key_rows), pos_bias, seg_count)
    prob_low = lowered(probability)
    value_pad = padded_segments(value_rows)
    attended = sum((jnp.einsum('cqk,ckd->cqd', prob_low[:, :, offset], value_pad[offset:offset + seg_count]) for offset in range(LEFT + 1)))
    return attended.reshape(-1, HEAD_DIM)

def backward_head(packed):
    query_rows, key_rows, value_rows, grad_rows, pos_bias = packed
    seg_count = query_rows.shape[0] // SEG
    query_seg = query_rows.astype(jnp.float32).reshape(seg_count, SEG, HEAD_DIM)
    key_pad = padded_segments(key_rows)
    value_pad = padded_segments(value_rows)
    probability = head_probs(query_seg, key_pad, pos_bias, seg_count)
    prob_low = lowered(probability)
    grad_seg = grad_rows.astype(jnp.float32).reshape(seg_count, SEG, HEAD_DIM)
    grad_probs = jnp.stack([jnp.einsum('cqd,ckd->cqk', grad_seg, value_pad[offset:offset + seg_count]) for offset in range(LEFT + 1)], axis=2)
    row_dot = lax.optimization_barrier(jnp.sum(probability * grad_probs, axis=(2, 3), keepdims=True))
    grad_scores = probability * (grad_probs - row_dot)
    grad_low = lowered(grad_scores)
    scale_root = math.sqrt(HEAD_DIM)
    grad_query = sum((jnp.einsum('cqk,ckd->cqd', grad_low[:, :, offset], key_pad[offset:offset + seg_count]) for offset in range(LEFT + 1))) / scale_root
    key_grad = jnp.zeros((seg_count + LEFT, SEG, HEAD_DIM), jnp.float32)
    value_grad = jnp.zeros((seg_count + LEFT, SEG, HEAD_DIM), jnp.float32)
    for offset in range(LEFT + 1):
        key_grad = key_grad.at[offset:offset + seg_count].add(jnp.einsum('cqk,cqd->ckd', grad_low[:, :, offset], query_seg))
        value_grad = value_grad.at[offset:offset + seg_count].add(jnp.einsum('cqk,cqd->ckd', prob_low[:, :, offset], grad_seg))
    return (grad_query.reshape(-1, HEAD_DIM).astype(jnp.bfloat16), (key_grad[LEFT:] / scale_root).reshape(-1, HEAD_DIM).astype(jnp.bfloat16), value_grad[LEFT:].reshape(-1, HEAD_DIM).astype(jnp.bfloat16), lax.optimization_barrier(jnp.sum(grad_scores, axis=0)))

def split_heads(array):
    return array.reshape(array.shape[0], HEADS, HEAD_DIM).transpose(1, 0, 2)

def merge_heads(array):
    return array.transpose(1, 0, 2).reshape(array.shape[1], HEADS * HEAD_DIM)

def reference(queries, key_vectors, value_vectors, cotangent, out_gain, rel_table):
    pos_bias, pullback = jax.vjp(expand_bias, rel_table.astype(jnp.float32))
    gain_rows = out_gain.astype(jnp.float32)

    def one_sequence(packed):
        query_seq, key_seq, value_seq, cot_seq = packed
        query_heads = split_heads(query_seq)
        key_heads = split_heads(key_seq)
        value_heads = split_heads(value_seq)
        attended = merge_heads(lax.map(forward_head, (query_heads, key_heads, value_heads, pos_bias)))
        inv_rms = lax.rsqrt(lax.optimization_barrier(jnp.mean(attended * attended, axis=-1, keepdims=True)) + epsilon)
        scaled = cot_seq.astype(jnp.float32) * gain_rows
        mean_prod = lax.optimization_barrier(jnp.mean(attended * scaled, axis=-1, keepdims=True))
        grad_attended = (inv_rms * scaled - attended * inv_rms ** 3 * mean_prod).astype(jnp.bfloat16)
        grad_query, grad_key, grad_value, bias_grad = lax.map(backward_head, (query_heads, key_heads, value_heads, split_heads(grad_attended), pos_bias))
        return (merge_heads(grad_query), merge_heads(grad_key), merge_heads(grad_value), bias_grad)
    grad_queries, grad_keys, grad_values, bias_grads = lax.map(one_sequence, (queries, key_vectors, value_vectors, cotangent))
    grad_table = pullback(lax.optimization_barrier(jnp.sum(bias_grads, axis=0)))[0]
    return (grad_queries, grad_keys, grad_values, grad_table)
```

```python
import functools
import math

import jax
import jax.numpy as jnp
from jax import lax
from jax.experimental import pallas as pl
from jax.experimental.pallas import tpu as pltpu
from jax.sharding import Mesh
from jax.sharding import PartitionSpec as P

HEAD_DIM = 128
SEG = 64
LEFT = 4
MAX_REL = 256
REL = 320
SP = ("sp_0", "sp_1")

PAIR = 2 * SEG
WINDOW = (LEFT + 2) * SEG
epsilon = 1e-06
masked_value = -1e30
f32 = jnp.float32
bf16 = jnp.bfloat16
exact = lax.Precision.HIGHEST
VMEM = pl.BlockSpec(memory_space=pltpu.VMEM)
SMEM = pl.BlockSpec(memory_space=pltpu.SMEM)


def dot(left, right, dims, precision=None):
    return lax.dot_general(
        left, right, (dims, ((), ())), preferred_element_type=f32, precision=precision
    )


def passed_along(block, axis, distance):
    devices = range(lax.axis_size(axis))
    route = [(i - distance, i) for i in devices if i - distance in devices]
    return lax.ppermute(block, axis, route)


def sent_to_all(copies, axis):
    return lax.all_to_all(copies, axis, split_axis=0, concat_axis=0, tiled=True)


def mirror(rows, cols):
    row_id = lax.broadcasted_iota(jnp.int32, (rows, cols), 0)
    col_id = lax.broadcasted_iota(jnp.int32, (rows, cols), 1)
    return row_id + col_id == REL - 1


def diagonal_sums(block):
    width = block.shape[1]
    folded = block[:8]
    for at in range(8, block.shape[0], 8):
        folded = folded + pltpu.roll(block[at : at + 8], width - at, 1)
    row = lax.broadcasted_iota(jnp.int32, folded.shape, 0)
    for step in (1, 2, 4):
        folded = jnp.where((row & step) != 0, pltpu.roll(folded, width - step, 1), folded)
    return jnp.sum(folded, axis=0, keepdims=True)


def bias_kernel(first_ref, rel_ref, bias_ref):
    heads, pairs = bias_ref.shape[:2]
    turned = dot(rel_ref[...], mirror(REL, WINDOW).astype(bf16), ((1,), (0,)))
    row = lax.broadcasted_iota(jnp.int32, (PAIR, WINDOW), 0)
    col = lax.broadcasted_iota(jnp.int32, (PAIR, WINDOW), 1)
    base = jnp.where(row >= SEG, SEG, 0)
    in_band = (col >= base) & (col < base + (LEFT + 1) * SEG)
    first = first_ref[0] == 1
    for h in range(heads):
        line = turned[h : h + 1]
        slid = pltpu.roll(jnp.broadcast_to(line, (PAIR, WINDOW)), 0, 1, stride=1, stride_axis=0)
        tile = jnp.where(col < row, jnp.broadcast_to(line[:, :1], (PAIR, WINDOW)), slid)
        tile = jnp.where(in_band, tile, masked_value)
        for g in range(pairs):
            start = jnp.where(first, LEFT * SEG - g * PAIR, 0)
            bias_ref[h, g] = jnp.where(col >= start, tile, masked_value)


def forward_kernel(
    q_ref, k_ref, v_ref, prior_ref, bias_ref, cot_ref, gain_ref, prob_ref, att_ref, stat_ref
):
    rows, width = q_ref.shape
    heads, pairs = width // HEAD_DIM, rows // PAIR
    scale_root = math.sqrt(HEAD_DIM)
    totals = None
    products = None
    ones = jnp.ones((8, HEAD_DIM), f32)
    for h in range(heads):
        ch = slice(h * HEAD_DIM, (h + 1) * HEAD_DIM)
        keys = jnp.concatenate([prior_ref[:rows, ch], k_ref[:, ch]], axis=0)
        values = jnp.concatenate([prior_ref[rows:, ch], v_ref[:, ch]], axis=0)
        outs = []
        for g in range(pairs):
            band = slice(g * PAIR, g * PAIR + WINDOW)
            here = slice(g * PAIR, (g + 1) * PAIR)
            scores = dot(q_ref[here, ch], keys[band], ((1,), (1,))) / scale_root + bias_ref[h, g]
            top = jnp.max(scores, axis=-1, keepdims=True)
            shifted = jnp.exp(scores - top)
            prob = shifted / jnp.sum(shifted, axis=-1, keepdims=True)
            prob_ref[h, g] = prob
            out = dot(prob.astype(bf16), values[band], ((1,), (0,)))
            att_ref[here, ch] = out
            outs.append(out)
        out = jnp.concatenate(outs, axis=0)
        scaled = cot_ref[:, ch].astype(f32) * gain_ref[:, ch].astype(f32)
        square = dot(ones, out * out, ((1,), (1,)), exact)
        product = dot(ones, out * scaled, ((1,), (1,)), exact)
        totals = square if totals is None else totals + square
        products = product if products is None else products + product
    half = rows // 2
    message = jnp.concatenate(
        [totals[:1, :half], totals[:1, half:], products[:1, :half], products[:1, half:]], axis=0
    )
    for d in range(stat_ref.shape[0]):
        stat_ref[d] = message


def backward_kernel(
    q_ref,
    k_ref,
    v_ref,
    prior_ref,
    cot_ref,
    gain_ref,
    prob_ref,
    att_ref,
    stat_ref,
    dq_ref,
    dk_ref,
    dv_ref,
    back_ref,
    table_ref,
    *,
    full_width,
):
    rows, width = q_ref.shape
    heads, pairs = width // HEAD_DIM, rows // PAIR
    half = rows // 2
    scale_root = math.sqrt(HEAD_DIM)
    summed = stat_ref[0]
    for d in range(1, stat_ref.shape[0]):
        summed = summed + stat_ref[d]
    pick = lax.broadcasted_iota(jnp.int32, (4, 4 * HEAD_DIM), 1) // HEAD_DIM
    pick = (pick == lax.broadcasted_iota(jnp.int32, (4, 4 * HEAD_DIM), 0)).astype(f32)
    spread = dot(summed, pick, ((0,), (0,)), exact)
    squares = jnp.concatenate([spread[:, :128], spread[:, 128:256]], axis=0)
    products = jnp.concatenate([spread[:, 256:384], spread[:, 384:]], axis=0)
    inv_rms = lax.rsqrt(squares / full_width + epsilon)
    pull = inv_rms**3 * (products / full_width)
    lines = []
    for h in range(heads):
        ch = slice(h * HEAD_DIM, (h + 1) * HEAD_DIM)
        keys = jnp.concatenate([prior_ref[:rows, ch], k_ref[:, ch]], axis=0)
        values = jnp.concatenate([prior_ref[rows:, ch], v_ref[:, ch]], axis=0)
        scaled = cot_ref[:, ch].astype(f32) * gain_ref[:, ch].astype(f32)
        grad = (inv_rms * scaled - att_ref[:, ch] * pull).astype(bf16)
        summed_scores = None
        key_parts = []
        value_parts = []
        for g in range(pairs):
            band = slice(g * PAIR, g * PAIR + WINDOW)
            here = slice(g * PAIR, (g + 1) * PAIR)
            prob = prob_ref[h, g]
            grad_probs = dot(grad[here], values[band], ((1,), (1,)))
            row_dot = jnp.sum(prob * grad_probs, axis=-1, keepdims=True)
            grad_scores = prob * (grad_probs - row_dot)
            grad_low = grad_scores.astype(bf16)
            summed_scores = grad_scores if summed_scores is None else summed_scores + grad_scores
            dq = dot(grad_low, keys[band], ((1,), (0,))) / scale_root
            dq_ref[here, ch] = dq.astype(bf16)
            key_parts.append(dot(grad_low, q_ref[here, ch], ((0,), (0,))))
            value_parts.append(dot(prob.astype(bf16), grad[here], ((0,), (0,))))
        lower = pltpu.roll(summed_scores[SEG:], WINDOW - SEG, 1)
        joined = summed_scores[:SEG] + lower
        lines.append(diagonal_sums(joined))
        for parts, back_at, own_ref, scale in (
            (key_parts, 0, dk_ref, scale_root),
            (value_parts, rows, dv_ref, 1.0),
        ):
            merged = []
            for block in range((rows + LEFT * SEG) // PAIR):
                total = None
                for g in range(pairs):
                    at = block - g
                    if 0 <= at < WINDOW // PAIR:
                        part = parts[g][at * PAIR : (at + 1) * PAIR]
                        total = part if total is None else total + part
                merged.append(total)
            merged = jnp.concatenate(merged, axis=0) / scale
            back_ref[back_at : back_at + rows, ch] = merged[: LEFT * SEG].astype(bf16)
            own_ref[:, ch] = merged[LEFT * SEG :]
    line = jnp.concatenate(lines, axis=0)
    col = lax.broadcasted_iota(jnp.int32, line.shape, 1)
    wrapped = jnp.sum(jnp.where(col > REL, line, 0.0), axis=1, keepdims=True)
    line = jnp.where(col == 0, line + wrapped, line)
    for h in range(heads):
        table_ref[:, :, h * REL : (h + 1) * REL] = jnp.broadcast_to(
            line[h : h + 1, :REL][None], (table_ref.shape[0], 1, REL)
        )


def final_kernel(dk_ref, dv_ref, back_ref, key_ref, value_ref):
    rows = dk_ref.shape[0]
    key_ref[...] = (dk_ref[...] + back_ref[:rows].astype(f32)).astype(bf16)
    value_ref[...] = (dv_ref[...] + back_ref[rows:].astype(f32)).astype(bf16)


def table_kernel(all_ref, table_ref):
    heads = table_ref.shape[0]
    total = jnp.sum(all_ref[...], axis=0)
    lines = jnp.concatenate([total[:, h * REL : (h + 1) * REL] for h in range(heads)], axis=0)
    table_ref[...] = dot(lines, mirror(REL, REL).astype(f32), ((1,), (0,)), exact)


def call(kernel, outs, in_specs=None, n_in=0):
    return pl.pallas_call(
        kernel,
        out_shape=outs,
        in_specs=in_specs or [VMEM] * n_in,
        out_specs=jax.tree.map(lambda _: VMEM, outs),
    )


def on_device(queries, key_vectors, value_vectors, cotangent, out_gain, rel_table):
    shape = queries.shape
    rows, width = shape[1], shape[2]
    heads, pairs = width // HEAD_DIM, rows // PAIR
    q, k, v, cot = (a.reshape(rows, width) for a in (queries, key_vectors, value_vectors, cotangent))
    gain = out_gain.reshape(1, width)
    members = lax.axis_size("tp")
    out = jax.ShapeDtypeStruct
    prior = passed_along(jnp.concatenate([k, v], axis=0), SP, 1)
    first = (lax.axis_index(SP) == 0).astype(jnp.int32).reshape(1)
    bias = call(bias_kernel, out((heads, pairs, PAIR, WINDOW), f32), [SMEM, VMEM])(first, rel_table)
    prob, att, stat = call(
        forward_kernel,
        (
            out((heads, pairs, PAIR, WINDOW), f32),
            out((rows, width), f32),
            out((members, 4, rows // 2), f32),
        ),
        n_in=7,
    )(q, k, v, prior, bias, cot, gain)
    stat = sent_to_all(stat, "tp")
    dq, dk, dv, back, table = call(
        functools.partial(backward_kernel, full_width=width * members),
        (
            out((rows, width), bf16),
            out((rows, width), f32),
            out((rows, width), f32),
            out((2 * rows, width), bf16),
            out((lax.axis_size(SP), 1, heads * REL), f32),
        ),
        n_in=9,
    )(q, k, v, prior, cot, gain, prob, att, stat)
    back = passed_along(back, SP, -1)
    table = sent_to_all(table, SP)
    grad_keys, grad_values = call(
        final_kernel, (out((rows, width), bf16), out((rows, width), bf16)), n_in=3
    )(dk, dv, back)
    grad_table = call(table_kernel, out((heads, REL), f32), n_in=1)(table)
    return (dq.reshape(shape), grad_keys.reshape(shape), grad_values.reshape(shape), grad_table)


def solution(mesh):
    finer = Mesh(mesh.devices.reshape(12, 8, mesh.shape["tp"]), ("sp_0", "sp_1", "tp"))
    placed = (
        P(None, SP, "tp"),
        P(None, SP, "tp"),
        P(None, SP, "tp"),
        P(None, SP, "tp"),
        P("tp"),
        P("tp", None),
    )
    return jax.shard_map(
        on_device,
        mesh=finer,
        in_specs=placed,
        out_specs=(P(None, SP, "tp"), P(None, SP, "tp"), P(None, SP, "tp"), P("tp", None)),
        check_vma=False,
    )
```

```python
import functools
import math

import jax
import jax.numpy as jnp
from jax import lax
from jax.experimental import pallas as pl
from jax.experimental.pallas import tpu as pltpu
from jax.sharding import Mesh
from jax.sharding import PartitionSpec as P


HEAD_DIM = 128
SEG = 64
LEFT = 4
REL = 320
SP = ("sp_0", "sp_1")

PAIR = 2 * SEG
PRIOR = LEFT * SEG
WINDOW = PRIOR + PAIR
ROOM = 12 * 1024 * 1024
epsilon = 1e-06
masked_value = -1e30
f32 = jnp.float32
bf16 = jnp.bfloat16
exact = lax.Precision.HIGHEST
kept = pltpu.VMEM
out = jax.ShapeDtypeStruct
VMEM = pl.BlockSpec(memory_space=pltpu.VMEM)
HBM = pl.BlockSpec(memory_space=pltpu.HBM)
SMEM = pl.BlockSpec(memory_space=pltpu.SMEM)


def dot(left, right, dims, precision=None):
    return lax.dot_general(
        left, right, (dims, ((), ())), preferred_element_type=f32, precision=precision
    )


def parts_of(array, count):
    found = []
    for _ in range(count):
        found.append(array.astype(bf16))
        array = array - found[-1].astype(f32)
    return found


def passed_along(block, axis, distance):
    devices = range(lax.axis_size(axis))
    route = [(i - distance, i) for i in devices if i - distance in devices]
    return lax.ppermute(block, axis, route)


def sent_to_all(copies, axis):
    return lax.all_to_all(copies, axis, split_axis=0, concat_axis=0, tiled=True)


def mirror(rows, cols):
    row_id = lax.broadcasted_iota(jnp.int32, (rows, cols), 0)
    col_id = lax.broadcasted_iota(jnp.int32, (rows, cols), 1)
    return row_id + col_id == REL - 1


def diagonal_sums(block):
    width = block.shape[1]
    folded = block[:8]
    for at in range(8, block.shape[0], 8):
        folded = folded + pltpu.roll(block[at : at + 8], width - at, 1)
    row = lax.broadcasted_iota(jnp.int32, folded.shape, 0)
    for step in (1, 2, 4):
        folded = jnp.where((row & step) != 0, pltpu.roll(folded, width - step, 1), folded)
    return jnp.sum(folded, axis=0, keepdims=True)


def head_of(h):
    return slice(h * HEAD_DIM, (h + 1) * HEAD_DIM)


def rows_of(g):
    return slice(g * PAIR, (g + 1) * PAIR)


def early_kernel(
    first_ref,
    rel_ref,
    gain_ref,
    q_hbm,
    k_hbm,
    cot_hbm,
    v_hbm,
    q_ref,
    k_ref,
    v_ref,
    own_ref,
    bias_ref,
    scaled_ref,
    cot_ref,
    sems,
):
    rows, width = q_ref.shape
    heads, pairs = width // HEAD_DIM, rows // PAIR
    scale = 1.0 / math.sqrt(HEAD_DIM)
    moves = ((q_hbm, q_ref), (k_hbm, k_ref), (cot_hbm, cot_ref), (v_hbm, v_ref))
    copies = [pltpu.make_async_copy(a, b, sems.at[i]) for i, (a, b) in enumerate(moves)]
    for copy in copies:
        copy.start()
    turned = dot(rel_ref[...], mirror(REL, WINDOW).astype(bf16), ((1,), (0,)))
    row = lax.broadcasted_iota(jnp.int32, (PAIR, WINDOW), 0)
    col = lax.broadcasted_iota(jnp.int32, (PAIR, WINDOW), 1)
    base = jnp.where(row >= SEG, SEG, 0)
    in_band = (col >= base) & (col < base + PRIOR + SEG)
    first = first_ref[0] == 1
    for h in range(heads):
        line = turned[h : h + 1]
        slid = pltpu.roll(jnp.broadcast_to(line, (PAIR, WINDOW)), 0, 1, stride=1, stride_axis=0)
        tile = jnp.where(col < row, jnp.broadcast_to(line[:, :1], (PAIR, WINDOW)), slid)
        tile = jnp.where(in_band, tile, masked_value)
        for g in range(pairs):
            split = PRIOR - g * PAIR
            prior = tile[:, :split]
            bias_ref[h, g, :, :split] = jnp.where(first, masked_value, prior)
            own_ref[h, g, :, split:] = tile[:, split:]
    copies[0].wait()
    copies[1].wait()
    for h in range(heads):
        for g in range(pairs):
            split = PRIOR - g * PAIR
            own = dot(q_ref[rows_of(g), head_of(h)], k_ref[: (g + 1) * PAIR, head_of(h)], ((1,), (1,)))
            own_ref[h, g, :, split:] += own * scale
    copies[2].wait()
    scaled_ref[...] = cot_ref[...].astype(f32) * gain_ref[...].astype(f32)
    copies[3].wait()


def forward_kernel(
    q_ref, v_ref, prior_key_ref, prior_value_ref, own_ref, bias_ref, scaled_ref, prob_ref, att_ref, stat_ref
):
    rows, width = q_ref.shape
    heads, pairs = width // HEAD_DIM, rows // PAIR
    scale = 1.0 / math.sqrt(HEAD_DIM)
    squares = None
    products = None
    for h in range(heads):
        ch = head_of(h)
        outs = []
        for g in range(pairs):
            here = rows_of(g)
            split = PRIOR - g * PAIR
            scores = dot(q_ref[here, ch], prior_key_ref[g * PAIR : PRIOR, ch], ((1,), (1,)))
            scores = scores * scale + bias_ref[h, g, :, :split]
            scores = jnp.concatenate([scores, own_ref[h, g, :, split:]], axis=1)
            top = jnp.max(scores, axis=-1, keepdims=True)
            shifted = jnp.exp(scores - top)
            prob = shifted * (1.0 / jnp.sum(shifted, axis=-1, keepdims=True))
            prob_ref[h, g] = prob
            values = jnp.concatenate(
                [prior_value_ref[g * PAIR :, ch], v_ref[: (g + 1) * PAIR, ch]], axis=0
            )
            attended = dot(prob.astype(bf16), values, ((1,), (0,)))
            att_ref[here, ch] = attended
            outs.append(attended)
        attended = jnp.concatenate(outs, axis=0)
        square = attended * attended
        product = attended * scaled_ref[:, ch]
        squares = square if squares is None else squares + square
        products = product if products is None else products + product
    lines = []
    ones = jnp.ones((8, 2 * HEAD_DIM), bf16)
    for total in (squares, products):
        lines.append(dot(ones, jnp.concatenate(parts_of(total, 2), axis=1), ((1,), (1,)))[:1])
    half = rows // 2
    message = jnp.concatenate([x[:, at : at + half] for x in lines for at in (0, half)], axis=0)
    for d in range(stat_ref.shape[0]):
        stat_ref[d] = message


def middle_kernel(
    v_ref,
    prior_value_ref,
    scaled_ref,
    prob_ref,
    att_ref,
    stat_ref,
    grad_ref,
    low_ref,
    table_ref,
    *,
    full_width,
):
    rows, width = v_ref.shape
    heads, pairs = width // HEAD_DIM, rows // PAIR
    summed = stat_ref[0]
    for d in range(1, stat_ref.shape[0]):
        summed = summed + stat_ref[d]
    pick = lax.broadcasted_iota(jnp.int32, (4, 4 * HEAD_DIM), 1) // HEAD_DIM
    pick = (pick == lax.broadcasted_iota(jnp.int32, (4, 4 * HEAD_DIM), 0)).astype(f32)
    spread = dot(summed, pick, ((0,), (0,)), exact)
    squares = jnp.concatenate([spread[:, :128], spread[:, 128:256]], axis=0)
    products = jnp.concatenate([spread[:, 256:384], spread[:, 384:]], axis=0)
    inv_rms = lax.rsqrt(squares * (1.0 / full_width) + epsilon)
    pull = inv_rms**3 * (products * (1.0 / full_width))
    lines = []
    for h in range(heads):
        ch = head_of(h)
        grad = (inv_rms * scaled_ref[:, ch] - att_ref[:, ch] * pull).astype(bf16)
        grad_ref[:, ch] = grad
        summed_scores = None
        for g in range(pairs):
            here = rows_of(g)
            prob = prob_ref[h, g]
            values = jnp.concatenate(
                [prior_value_ref[g * PAIR :, ch], v_ref[: (g + 1) * PAIR, ch]], axis=0
            )
            grad_probs = dot(grad[here], values, ((1,), (1,)))
            row_dot = jnp.sum(prob * grad_probs, axis=-1, keepdims=True)
            grad_scores = prob * (grad_probs - row_dot)
            grad_low = grad_scores.astype(bf16)
            low_ref[h, g] = grad_low
            summed_scores = grad_scores if summed_scores is None else summed_scores + grad_scores
        lower = pltpu.roll(summed_scores[SEG:], WINDOW - SEG, 1)
        lines.append(diagonal_sums(summed_scores[:SEG] + lower))
    line = jnp.concatenate(lines, axis=0)
    col = lax.broadcasted_iota(jnp.int32, line.shape, 1)
    wrapped = jnp.sum(jnp.where(col > REL, line, 0.0), axis=1, keepdims=True)
    line = jnp.where(col == 0, line + wrapped, line)
    table_ref[...] = jnp.broadcast_to(line[:, :REL].astype(bf16)[None], table_ref.shape)


def back_kernel(q_ref, prob_ref, grad_ref, low_ref, back_ref):
    rows, width = q_ref.shape
    heads, pairs = width // HEAD_DIM, rows // PAIR
    scale = 1.0 / math.sqrt(HEAD_DIM)
    for h in range(heads):
        ch = head_of(h)
        key_back = []
        value_back = []
        for g in range(pairs):
            here = rows_of(g)
            split = PRIOR - g * PAIR
            key_back.append(dot(low_ref[h, g, :, :split], q_ref[here, ch], ((0,), (0,))))
            prob = prob_ref[h, g, :, :split].astype(bf16)
            value_back.append(dot(prob, grad_ref[here, ch], ((0,), (0,))))
        for parts, back_at, factor in ((key_back, 0, scale), (value_back, PRIOR, 1.0)):
            for g in range(pairs):
                total = sum(
                    (parts[a][(g - a) * PAIR : (g - a + 1) * PAIR] for a in range(1, g + 1)),
                    parts[0][rows_of(g)],
                )
                at = back_at + g * PAIR
                back_ref[at : at + PAIR, ch] = (total * factor).astype(bf16)


def late_kernel(q_ref, k_ref, prior_key_ref, prob_ref, grad_ref, low_ref, dq_ref, dk_ref, dv_ref):
    rows, width = q_ref.shape
    heads, pairs = width // HEAD_DIM, rows // PAIR
    scale = 1.0 / math.sqrt(HEAD_DIM)
    for h in range(heads):
        ch = head_of(h)
        key_own = []
        value_own = []
        for g in range(pairs):
            here = rows_of(g)
            split = PRIOR - g * PAIR
            low = low_ref[h, g]
            keys = jnp.concatenate(
                [prior_key_ref[g * PAIR : PRIOR, ch], k_ref[: (g + 1) * PAIR, ch]], axis=0
            )
            dq_ref[here, ch] = (dot(low, keys, ((1,), (0,))) * scale).astype(bf16)
            key_own.append(dot(low[:, split:], q_ref[here, ch], ((0,), (0,))))
            prob = prob_ref[h, g, :, split:].astype(bf16)
            value_own.append(dot(prob, grad_ref[here, ch], ((0,), (0,))))
        for parts, own_ref, factor in ((key_own, dk_ref, scale), (value_own, dv_ref, 1.0)):
            for g in range(pairs):
                total = sum(
                    (parts[a][rows_of(g)] for a in range(g + 1, pairs)), parts[g][rows_of(g)]
                )
                own_ref[rows_of(g), ch] = total * factor


def final_kernel(dk_ref, dv_ref, back_ref, key_ref, value_ref):
    rows = dk_ref.shape[0]
    key_ref[...] = (dk_ref[...] + back_ref[:rows].astype(f32)).astype(bf16)
    value_ref[...] = (dv_ref[...] + back_ref[rows:].astype(f32)).astype(bf16)


def table_kernel(all_ref, table_ref):
    lines = jnp.sum(all_ref[...].astype(f32), axis=0)
    turn = mirror(REL, REL).astype(bf16)
    table_ref[...] = sum(dot(part, turn, ((1,), (0,))) for part in parts_of(lines, 3)[::-1])


def near(array):
    return pltpu.with_memory_space_constraint(array, pltpu.VMEM)


def far(array):
    return pltpu.with_memory_space_constraint(array, pltpu.HBM)


def call(kernel, outs, *arrays, scalars=0):
    many = isinstance(outs, tuple)
    return pl.pallas_call(
        kernel,
        out_shape=outs,
        in_specs=[SMEM] * scalars + [VMEM] * (len(arrays) - scalars),
        out_specs=(VMEM,) * len(outs) if many else VMEM,
        compiler_params=pltpu.CompilerParams(vmem_limit_bytes=ROOM),
    )(*arrays[:scalars], *(near(a) for a in arrays[scalars:]))


def on_device(queries, key_vectors, value_vectors, cotangent, out_gain, rel_table):
    shape = queries.shape
    rows, width = shape[1], shape[2]
    heads, pairs = width // HEAD_DIM, rows // PAIR
    q, k, v, cot = (a.reshape(rows, width) for a in (queries, key_vectors, value_vectors, cotangent))
    gain = out_gain.reshape(1, width)
    members = lax.axis_size("tp")
    tiles = (heads, pairs, PAIR, WINDOW)
    prior_keys = passed_along(k, SP, 1)
    prior_values = passed_along(v, SP, 1)
    first = (lax.axis_index(SP) == 0).astype(jnp.int32).reshape(1)
    own_block = kept((rows, width), bf16)
    q, k, v, own, bias, scaled = pl.pallas_call(
        early_kernel,
        out_shape=(own_block,) * 3 + (kept(tiles, f32), kept(tiles, f32), kept((rows, width), f32)),
        in_specs=[SMEM, VMEM, VMEM] + [HBM] * 4,
        out_specs=(VMEM,) * 6,
        scratch_shapes=[pltpu.VMEM((rows, width), bf16), pltpu.SemaphoreType.DMA((4,))],
        compiler_params=pltpu.CompilerParams(vmem_limit_bytes=ROOM),
    )(first, near(rel_table), near(gain), *(far(a) for a in (q, k, cot, v)))
    prob, att, stat = call(
        forward_kernel,
        (kept(tiles, f32), kept((rows, width), f32), kept((members, 4, rows // 2), f32)),
        *(q, v, prior_keys, prior_values, own, bias, scaled),
    )
    stat = sent_to_all(stat, "tp")
    grad, low, table = call(
        functools.partial(middle_kernel, full_width=width * members),
        (
            kept((rows, width), bf16),
            kept(tiles, bf16),
            kept((lax.axis_size(SP), heads, REL), bf16),
        ),
        *(v, prior_values, scaled, prob, att, stat),
    )
    table = sent_to_all(table, SP)
    back = call(back_kernel, kept((2 * rows, width), bf16), q, prob, grad, low)
    back = passed_along(back, SP, -1)
    dq, dk, dv = call(
        late_kernel,
        (out((rows, width), bf16), kept((rows, width), f32), kept((rows, width), f32)),
        *(q, k, prior_keys, prob, grad, low),
    )
    grad_keys, grad_values = call(
        final_kernel, (out((rows, width), bf16), out((rows, width), bf16)), dk, dv, back
    )
    grad_table = call(table_kernel, out((heads, REL), f32), table)
    return (dq.reshape(shape), grad_keys.reshape(shape), grad_values.reshape(shape), grad_table)


def solution(mesh):
    finer = Mesh(mesh.devices.reshape(12, 8, mesh.shape["tp"]), ("sp_0", "sp_1", "tp"))
    placed = (
        P(None, SP, "tp"),
        P(None, SP, "tp"),
        P(None, SP, "tp"),
        P(None, SP, "tp"),
        P("tp"),
        P("tp", None),
    )
    return jax.shard_map(
        on_device,
        mesh=finer,
        in_specs=placed,
        out_specs=(P(None, SP, "tp"), P(None, SP, "tp"), P(None, SP, "tp"), P("tp", None)),
        check_vma=False,
    )
```

```python
import functools
import math

import jax
import jax.numpy as jnp
from jax import lax
from jax.experimental import pallas as pl
from jax.experimental.pallas import tpu as pltpu
from jax.sharding import PartitionSpec as P


HEAD_DIM = 128
SEG = 64
LEFT = 4
REL = 320
SP = "sp"
LEADER = (9, 4, 7)

PAIR = 2 * SEG
PRIOR = LEFT * SEG
WINDOW = PRIOR + PAIR
ROOM = 12 * 1024 * 1024
epsilon = 1e-06
masked_value = -1e30
f32 = jnp.float32
bf16 = jnp.bfloat16
kept = pltpu.VMEM
out = jax.ShapeDtypeStruct
VMEM = pl.BlockSpec(memory_space=pltpu.VMEM)
HBM = pl.BlockSpec(memory_space=pltpu.HBM)
SMEM = pl.BlockSpec(memory_space=pltpu.SMEM)


def dot(left, right, dims):
    return lax.dot_general(left, right, (dims, ((), ())), preferred_element_type=f32)


def parts_of(array, count):
    found = []
    for _ in range(count):
        found.append(array.astype(bf16))
        array = array - found[-1].astype(f32)
    return found


def passed_along(block, axis, distance):
    devices = range(lax.axis_size(axis))
    route = [(i - distance, i) for i in devices if i - distance in devices]
    return lax.ppermute(block, axis, route)


def ahead(group, leader):
    return [group[leader]] + group[:leader] + group[leader + 1 :]


def sent_to_all(copies, axis, order):
    return lax.all_to_all(
        copies, axis, split_axis=0, concat_axis=0, tiled=True, axis_index_groups=order
    )


def mirror(rows, cols):
    row_id = lax.broadcasted_iota(jnp.int32, (rows, cols), 0)
    col_id = lax.broadcasted_iota(jnp.int32, (rows, cols), 1)
    return row_id + col_id == REL - 1


def diagonal_sums(block):
    width = block.shape[1]
    folded = block[:8]
    for at in range(8, block.shape[0], 8):
        folded = folded + pltpu.roll(block[at : at + 8], width - at, 1)
    row = lax.broadcasted_iota(jnp.int32, folded.shape, 0)
    for step in (1, 2, 4):
        folded = jnp.where((row & step) != 0, pltpu.roll(folded, width - step, 1), folded)
    return jnp.sum(folded, axis=0, keepdims=True)


def head_of(h):
    return slice(h * HEAD_DIM, (h + 1) * HEAD_DIM)


def rows_of(g):
    return slice(g * PAIR, (g + 1) * PAIR)


def early_kernel(
    first_ref,
    rel_ref,
    gain_ref,
    q_hbm,
    k_hbm,
    cot_hbm,
    v_hbm,
    q_ref,
    k_ref,
    v_ref,
    own_ref,
    bias_ref,
    scaled_ref,
    turn_ref,
    cot_ref,
    sems,
):
    rows, width = q_ref.shape
    heads, pairs = width // HEAD_DIM, rows // PAIR
    scale = 1.0 / math.sqrt(HEAD_DIM)
    moves = ((q_hbm, q_ref), (k_hbm, k_ref), (cot_hbm, cot_ref), (v_hbm, v_ref))
    copies = [pltpu.make_async_copy(a, b, sems.at[i]) for i, (a, b) in enumerate(moves)]
    for copy in copies:
        copy.start()
    turn_ref[...] = mirror(REL, REL).astype(bf16)
    turned = dot(rel_ref[...], mirror(REL, WINDOW).astype(bf16), ((1,), (0,)))
    row = lax.broadcasted_iota(jnp.int32, (PAIR, WINDOW), 0)
    col = lax.broadcasted_iota(jnp.int32, (PAIR, WINDOW), 1)
    base = jnp.where(row >= SEG, SEG, 0)
    in_band = (col >= base) & (col < base + PRIOR + SEG)
    first = first_ref[0] == 1
    for h in range(heads):
        line = turned[h : h + 1]
        slid = pltpu.roll(jnp.broadcast_to(line, (PAIR, WINDOW)), 0, 1, stride=1, stride_axis=0)
        tile = jnp.where(col < row, jnp.broadcast_to(line[:, :1], (PAIR, WINDOW)), slid)
        tile = jnp.where(in_band, tile, masked_value)
        for g in range(pairs):
            split = PRIOR - g * PAIR
            prior = tile[:, :split]
            bias_ref[h, g, :, :split] = jnp.where(first, masked_value, prior)
            own_ref[h, g, :, split:] = tile[:, split:]
    copies[0].wait()
    copies[1].wait()
    for h in range(heads):
        for g in range(pairs):
            split = PRIOR - g * PAIR
            own = dot(q_ref[rows_of(g), head_of(h)], k_ref[: (g + 1) * PAIR, head_of(h)], ((1,), (1,)))
            own_ref[h, g, :, split:] += own * scale
    copies[2].wait()
    scaled_ref[...] = cot_ref[...].astype(f32) * gain_ref[...].astype(f32)
    copies[3].wait()


def forward_kernel(
    q_ref, v_ref, prior_key_ref, prior_value_ref, own_ref, bias_ref, scaled_ref, prob_ref, att_ref, stat_ref
):
    rows, width = q_ref.shape
    heads, pairs = width // HEAD_DIM, rows // PAIR
    scale = 1.0 / math.sqrt(HEAD_DIM)
    squares = None
    products = None
    for h in range(heads):
        ch = head_of(h)
        outs = []
        for g in range(pairs):
            here = rows_of(g)
            split = PRIOR - g * PAIR
            scores = dot(q_ref[here, ch], prior_key_ref[g * PAIR : PRIOR, ch], ((1,), (1,)))
            scores = scores * scale + bias_ref[h, g, :, :split]
            scores = jnp.concatenate([scores, own_ref[h, g, :, split:]], axis=1)
            top = jnp.max(scores, axis=-1, keepdims=True)
            shifted = jnp.exp(scores - top)
            prob = shifted * (1.0 / jnp.sum(shifted, axis=-1, keepdims=True))
            prob_ref[h, g] = prob
            values = jnp.concatenate(
                [prior_value_ref[g * PAIR :, ch], v_ref[: (g + 1) * PAIR, ch]], axis=0
            )
            attended = dot(prob.astype(bf16), values, ((1,), (0,)))
            att_ref[here, ch] = attended
            outs.append(attended)
        attended = jnp.concatenate(outs, axis=0)
        square = attended * attended
        product = attended * scaled_ref[:, ch]
        squares = square if squares is None else squares + square
        products = product if products is None else products + product
    lines = []
    ones = jnp.ones((8, 2 * HEAD_DIM), bf16)
    for total in (squares, products):
        lines.append(dot(ones, jnp.concatenate(parts_of(total, 2), axis=1), ((1,), (1,)))[:1])
    half = rows // 2
    message = jnp.concatenate([x[:, at : at + half] for x in lines for at in (0, half)], axis=0)
    for d in range(stat_ref.shape[0]):
        stat_ref[d] = message


def middle_kernel(
    v_ref,
    prior_value_ref,
    scaled_ref,
    prob_ref,
    att_ref,
    stat_ref,
    grad_ref,
    low_ref,
    table_ref,
    *,
    full_width,
):
    rows, width = v_ref.shape
    heads, pairs = width // HEAD_DIM, rows // PAIR
    summed = stat_ref[0]
    for d in range(1, stat_ref.shape[0]):
        summed = summed + stat_ref[d]
    pieces = jnp.concatenate(parts_of(summed, 3), axis=0)
    pick = lax.broadcasted_iota(jnp.int32, (12, 4 * HEAD_DIM), 1) // HEAD_DIM
    pick = (pick == lax.broadcasted_iota(jnp.int32, (12, 4 * HEAD_DIM), 0) % 4).astype(bf16)
    spread = dot(pieces, pick, ((0,), (0,)))
    squares = jnp.concatenate([spread[:, :128], spread[:, 128:256]], axis=0)
    products = jnp.concatenate([spread[:, 256:384], spread[:, 384:]], axis=0)
    inv_rms = lax.rsqrt(squares * (1.0 / full_width) + epsilon)
    pull = inv_rms**3 * (products * (1.0 / full_width))
    lines = []
    for h in range(heads):
        ch = head_of(h)
        grad = (inv_rms * scaled_ref[:, ch] - att_ref[:, ch] * pull).astype(bf16)
        grad_ref[:, ch] = grad
        summed_scores = None
        for g in range(pairs):
            here = rows_of(g)
            prob = prob_ref[h, g]
            values = jnp.concatenate(
                [prior_value_ref[g * PAIR :, ch], v_ref[: (g + 1) * PAIR, ch]], axis=0
            )
            grad_probs = dot(grad[here], values, ((1,), (1,)))
            row_dot = jnp.sum(prob * grad_probs, axis=-1, keepdims=True)
            grad_scores = prob * (grad_probs - row_dot)
            grad_low = grad_scores.astype(bf16)
            low_ref[h, g] = grad_low
            summed_scores = grad_scores if summed_scores is None else summed_scores + grad_scores
        lower = pltpu.roll(summed_scores[SEG:], WINDOW - SEG, 1)
        lines.append(diagonal_sums(summed_scores[:SEG] + lower))
    line = jnp.concatenate(lines, axis=0)
    col = lax.broadcasted_iota(jnp.int32, line.shape, 1)
    wrapped = jnp.sum(jnp.where(col > REL, line, 0.0), axis=1, keepdims=True)
    line = jnp.where(col == 0, line + wrapped, line)
    table_ref[...] = jnp.broadcast_to(line[:, :REL][None], table_ref.shape)


def back_kernel(q_ref, prob_ref, grad_ref, low_ref, back_ref):
    rows, width = q_ref.shape
    heads, pairs = width // HEAD_DIM, rows // PAIR
    scale = 1.0 / math.sqrt(HEAD_DIM)
    for h in range(heads):
        ch = head_of(h)
        key_back = []
        value_back = []
        for g in range(pairs):
            here = rows_of(g)
            split = PRIOR - g * PAIR
            key_back.append(dot(low_ref[h, g, :, :split], q_ref[here, ch], ((0,), (0,))))
            prob = prob_ref[h, g, :, :split].astype(bf16)
            value_back.append(dot(prob, grad_ref[here, ch], ((0,), (0,))))
        for parts, back_at, factor in ((key_back, 0, scale), (value_back, PRIOR, 1.0)):
            for g in range(pairs):
                total = sum(
                    (parts[a][(g - a) * PAIR : (g - a + 1) * PAIR] for a in range(1, g + 1)),
                    parts[0][rows_of(g)],
                )
                at = back_at + g * PAIR
                back_ref[at : at + PAIR, ch] = (total * factor).astype(bf16)


def late_kernel(q_ref, k_ref, prior_key_ref, prob_ref, grad_ref, low_ref, dq_ref, dk_ref, dv_ref):
    rows, width = q_ref.shape
    heads, pairs = width // HEAD_DIM, rows // PAIR
    scale = 1.0 / math.sqrt(HEAD_DIM)
    for h in range(heads):
        ch = head_of(h)
        key_own = []
        value_own = []
        for g in range(pairs):
            here = rows_of(g)
            split = PRIOR - g * PAIR
            low = low_ref[h, g]
            keys = jnp.concatenate(
                [prior_key_ref[g * PAIR : PRIOR, ch], k_ref[: (g + 1) * PAIR, ch]], axis=0
            )
            dq_ref[here, ch] = (dot(low, keys, ((1,), (0,))) * scale).astype(bf16)
            key_own.append(dot(low[:, split:], q_ref[here, ch], ((0,), (0,))))
            prob = prob_ref[h, g, :, split:].astype(bf16)
            value_own.append(dot(prob, grad_ref[here, ch], ((0,), (0,))))
        for parts, own_ref, factor in ((key_own, dk_ref, scale), (value_own, dv_ref, 1.0)):
            for g in range(pairs):
                total = sum(
                    (parts[a][rows_of(g)] for a in range(g + 1, pairs)), parts[g][rows_of(g)]
                )
                own_ref[rows_of(g), ch] = total * factor


def final_kernel(dk_ref, dv_ref, back_ref, key_ref, value_ref):
    rows = dk_ref.shape[0]
    key_ref[...] = (dk_ref[...] + back_ref[:rows].astype(f32)).astype(bf16)
    value_ref[...] = (dv_ref[...] + back_ref[rows:].astype(f32)).astype(bf16)


def relay_kernel(all_ref, out_ref):
    out_ref[...] = jnp.broadcast_to(jnp.sum(all_ref[...], axis=0)[None], out_ref.shape)


def table_kernel(all_ref, turn_ref, table_ref):
    heads = table_ref.shape[0]
    pieces = jnp.concatenate(parts_of(jnp.sum(all_ref[...], axis=0), 3), axis=0)
    lines = dot(pieces, turn_ref[...], ((1,), (0,)))
    table_ref[...] = lines[2 * heads :] + lines[heads : 2 * heads] + lines[:heads]


def near(array):
    return pltpu.with_memory_space_constraint(array, pltpu.VMEM)


def far(array):
    return pltpu.with_memory_space_constraint(array, pltpu.HBM)


def call(kernel, outs, *arrays, scalars=0):
    many = isinstance(outs, tuple)
    return pl.pallas_call(
        kernel,
        out_shape=outs,
        in_specs=[SMEM] * scalars + [VMEM] * (len(arrays) - scalars),
        out_specs=(VMEM,) * len(outs) if many else VMEM,
        compiler_params=pltpu.CompilerParams(vmem_limit_bytes=ROOM),
    )(*arrays[:scalars], *(near(a) for a in arrays[scalars:]))


def on_device(queries, key_vectors, value_vectors, cotangent, out_gain, rel_table):
    shape = queries.shape
    rows, width = shape[1], shape[2]
    heads, pairs = width // HEAD_DIM, rows // PAIR
    q, k, v, cot = (a.reshape(rows, width) for a in (queries, key_vectors, value_vectors, cotangent))
    gain = out_gain.reshape(1, width)
    members = lax.axis_size("tp")
    tiles = (heads, pairs, PAIR, WINDOW)
    prior_keys = passed_along(k, SP, 1)
    prior_values = passed_along(v, SP, 1)
    first = (lax.axis_index(SP) == 0).astype(jnp.int32).reshape(1)
    own_block = kept((rows, width), bf16)
    q, k, v, own, bias, scaled, turn = pl.pallas_call(
        early_kernel,
        out_shape=(own_block,) * 3
        + (kept(tiles, f32), kept(tiles, f32), kept((rows, width), f32), kept((REL, REL), bf16)),
        in_specs=[SMEM, VMEM, VMEM] + [HBM] * 4,
        out_specs=(VMEM,) * 7,
        scratch_shapes=[pltpu.VMEM((rows, width), bf16), pltpu.SemaphoreType.DMA((4,))],
        compiler_params=pltpu.CompilerParams(vmem_limit_bytes=ROOM),
    )(first, near(rel_table), near(gain), *(far(a) for a in (q, k, cot, v)))
    prob, att, stat = call(
        forward_kernel,
        (kept(tiles, f32), kept((rows, width), f32), kept((members, 4, rows // 2), f32)),
        *(q, v, prior_keys, prior_values, own, bias, scaled),
    )
    stat = sent_to_all(stat, "tp", [ahead(list(range(members)), LEADER[2])])
    grad, low, table = call(
        functools.partial(middle_kernel, full_width=width * members),
        (
            kept((rows, width), bf16),
            kept(tiles, bf16),
            kept((8, heads, REL), f32),
        ),
        *(v, prior_values, scaled, prob, att, stat),
    )
    order = [ahead([z * 8 + y for y in range(8)], LEADER[1]) for z in range(12)]
    table = sent_to_all(table, SP, order)
    table = call(relay_kernel, kept((12, heads, REL), f32), table)
    order = [ahead([z * 8 + y for z in range(12)], LEADER[0]) for y in range(8)]
    table = sent_to_all(table, SP, order)
    back = call(back_kernel, kept((2 * rows, width), bf16), q, prob, grad, low)
    back = passed_along(back, SP, -1)
    dq, dk, dv = call(
        late_kernel,
        (out((rows, width), bf16), kept((rows, width), f32), kept((rows, width), f32)),
        *(q, k, prior_keys, prob, grad, low),
    )
    grad_keys, grad_values = call(
        final_kernel, (out((rows, width), bf16), out((rows, width), bf16)), dk, dv, back
    )
    grad_table = call(table_kernel, out((heads, REL), f32), table, turn)
    return (dq.reshape(shape), grad_keys.reshape(shape), grad_values.reshape(shape), grad_table)


def solution(mesh):
    placed = (
        P(None, SP, "tp"),
        P(None, SP, "tp"),
        P(None, SP, "tp"),
        P(None, SP, "tp"),
        P("tp"),
        P("tp", None),
    )
    return jax.shard_map(
        on_device,
        mesh=mesh,
        in_specs=placed,
        out_specs=(P(None, SP, "tp"), P(None, SP, "tp"), P(None, SP, "tp"), P("tp", None)),
        check_vma=False,
    )
```

```python
import functools
import math

import jax
import jax.numpy as jnp
from jax import lax
from jax.experimental import pallas as pl
from jax.experimental.pallas import tpu as pltpu
from jax.sharding import PartitionSpec as P


HEAD_DIM = 128
SEG = 64
LEFT = 4
REL = 320
SP = "sp"
LEADER = (9, 4, 7)

PAIR = 2 * SEG
PRIOR = LEFT * SEG
WINDOW = PRIOR + PAIR
ROOM = 12 * 1024 * 1024
epsilon = 1e-06
masked_value = -1e30
f32 = jnp.float32
bf16 = jnp.bfloat16
kept = pltpu.VMEM
out = jax.ShapeDtypeStruct
VMEM = pl.BlockSpec(memory_space=pltpu.VMEM)
HBM = pl.BlockSpec(memory_space=pltpu.HBM)
SMEM = pl.BlockSpec(memory_space=pltpu.SMEM)


def dot(left, right, dims):
    return lax.dot_general(left, right, (dims, ((), ())), preferred_element_type=f32)


def parts_of(array, count):
    found = []
    for _ in range(count):
        found.append(array.astype(bf16))
        array = array - found[-1].astype(f32)
    return found


def passed_along(block, axis, distance):
    devices = range(lax.axis_size(axis))
    route = [(i - distance, i) for i in devices if i - distance in devices]
    return lax.ppermute(block, axis, route)


def ahead(group, leader):
    return [group[leader]] + group[:leader] + group[leader + 1 :]


def sent_to_all(copies, axis, order):
    return lax.all_to_all(
        copies, axis, split_axis=0, concat_axis=0, tiled=True, axis_index_groups=order
    )


def mirror(rows, cols):
    row_id = lax.broadcasted_iota(jnp.int32, (rows, cols), 0)
    col_id = lax.broadcasted_iota(jnp.int32, (rows, cols), 1)
    return row_id + col_id == REL - 1


def diagonal_sums(block):
    width = block.shape[1]
    folded = block[:8]
    for at in range(8, block.shape[0], 8):
        folded = folded + pltpu.roll(block[at : at + 8], width - at, 1)
    row = lax.broadcasted_iota(jnp.int32, folded.shape, 0)
    for step in (1, 2, 4):
        folded = jnp.where((row & step) != 0, pltpu.roll(folded, width - step, 1), folded)
    return jnp.sum(folded, axis=0, keepdims=True)


def head_of(h):
    return slice(h * HEAD_DIM, (h + 1) * HEAD_DIM)


def rows_of(g):
    return slice(g * PAIR, (g + 1) * PAIR)


def early_kernel(
    first_ref,
    rel_ref,
    gain_ref,
    q_hbm,
    k_hbm,
    cot_hbm,
    v_hbm,
    q_ref,
    k_ref,
    v_ref,
    own_ref,
    bias_ref,
    scaled_ref,
    turn_ref,
    cot_ref,
    sems,
):
    rows, width = q_ref.shape
    heads, pairs = width // HEAD_DIM, rows // PAIR
    scale = 1.0 / math.sqrt(HEAD_DIM)
    moves = ((q_hbm, q_ref), (k_hbm, k_ref), (cot_hbm, cot_ref), (v_hbm, v_ref))
    copies = [pltpu.make_async_copy(a, b, sems.at[i]) for i, (a, b) in enumerate(moves)]
    for copy in copies:
        copy.start()
    turn_ref[...] = mirror(REL, REL).astype(bf16)
    turned = dot(rel_ref[...], mirror(REL, WINDOW).astype(bf16), ((1,), (0,)))
    row = lax.broadcasted_iota(jnp.int32, (PAIR, WINDOW), 0)
    col = lax.broadcasted_iota(jnp.int32, (PAIR, WINDOW), 1)
    base = jnp.where(row >= SEG, SEG, 0)
    in_band = (col >= base) & (col < base + PRIOR + SEG)
    first = first_ref[0] == 1
    for h in range(heads):
        line = turned[h : h + 1]
        slid = pltpu.roll(jnp.broadcast_to(line, (PAIR, WINDOW)), 0, 1, stride=1, stride_axis=0)
        tile = jnp.where(col < row, jnp.broadcast_to(line[:, :1], (PAIR, WINDOW)), slid)
        tile = jnp.where(in_band, tile, masked_value)
        for g in range(pairs):
            split = PRIOR - g * PAIR
            prior = tile[:, :split]
            bias_ref[h, g, :, :split] = jnp.where(first, masked_value, prior)
            own_ref[h, g, :, split:] = tile[:, split:]
    copies[0].wait()
    copies[1].wait()
    for h in range(heads):
        for g in range(pairs):
            split = PRIOR - g * PAIR
            own = dot(q_ref[rows_of(g), head_of(h)], k_ref[: (g + 1) * PAIR, head_of(h)], ((1,), (1,)))
            own_ref[h, g, :, split:] += own * scale
    copies[2].wait()
    scaled_ref[...] = cot_ref[...].astype(f32) * gain_ref[...].astype(f32)
    copies[3].wait()


def weights_kernel(q_ref, prior_key_ref, own_ref, bias_ref, prob_ref, weight_ref):
    heads, pairs = prob_ref.shape[:2]
    scale = 1.0 / math.sqrt(HEAD_DIM)
    for h in range(heads):
        for g in range(pairs):
            split = PRIOR - g * PAIR
            keys = prior_key_ref[g * PAIR : PRIOR, head_of(h)]
            scores = dot(q_ref[rows_of(g), head_of(h)], keys, ((1,), (1,)))
            scores = scores * scale + bias_ref[h, g, :, :split]
            scores = jnp.concatenate([scores, own_ref[h, g, :, split:]], axis=1)
            top = jnp.max(scores, axis=-1, keepdims=True)
            shifted = jnp.exp(scores - top)
            prob = shifted * (1.0 / jnp.sum(shifted, axis=-1, keepdims=True))
            prob_ref[h, g] = prob
            weight_ref[h, g] = prob.astype(bf16)


def forward_kernel(weight_ref, v_ref, prior_value_ref, scaled_ref, att_ref, stat_ref):
    rows, width = v_ref.shape
    heads, pairs = width // HEAD_DIM, rows // PAIR
    squares = None
    products = None
    for h in range(heads):
        ch = head_of(h)
        outs = []
        for g in range(pairs):
            values = jnp.concatenate(
                [prior_value_ref[g * PAIR :, ch], v_ref[: (g + 1) * PAIR, ch]], axis=0
            )
            outs.append(dot(weight_ref[h, g], values, ((1,), (0,))))
        attended = jnp.concatenate(outs, axis=0)
        att_ref[:, ch] = attended
        square = attended * attended
        product = attended * scaled_ref[:, ch]
        squares = square if squares is None else squares + square
        products = product if products is None else products + product
    lines = []
    ones = jnp.ones((8, 2 * HEAD_DIM), bf16)
    for total in (squares, products):
        lines.append(dot(ones, jnp.concatenate(parts_of(total, 2), axis=1), ((1,), (1,)))[:1])
    half = rows // 2
    message = jnp.concatenate([x[:, at : at + half] for x in lines for at in (0, half)], axis=0)
    for d in range(stat_ref.shape[0]):
        stat_ref[d] = message


def middle_kernel(
    v_ref,
    prior_value_ref,
    scaled_ref,
    prob_ref,
    att_ref,
    stat_ref,
    grad_ref,
    low_ref,
    table_ref,
    *,
    full_width,
):
    rows, width = v_ref.shape
    heads, pairs = width // HEAD_DIM, rows // PAIR
    summed = stat_ref[0]
    for d in range(1, stat_ref.shape[0]):
        summed = summed + stat_ref[d]
    pieces = jnp.concatenate(parts_of(summed, 3), axis=0)
    pick = lax.broadcasted_iota(jnp.int32, (12, 4 * HEAD_DIM), 1) // HEAD_DIM
    pick = (pick == lax.broadcasted_iota(jnp.int32, (12, 4 * HEAD_DIM), 0) % 4).astype(bf16)
    spread = dot(pieces, pick, ((0,), (0,)))
    squares = jnp.concatenate([spread[:, :128], spread[:, 128:256]], axis=0)
    products = jnp.concatenate([spread[:, 256:384], spread[:, 384:]], axis=0)
    inv_rms = lax.rsqrt(squares * (1.0 / full_width) + epsilon)
    pull = inv_rms**3 * (products * (1.0 / full_width))
    lines = []
    for h in range(heads):
        ch = head_of(h)
        grad = (inv_rms * scaled_ref[:, ch] - att_ref[:, ch] * pull).astype(bf16)
        grad_ref[:, ch] = grad
        summed_scores = None
        for g in range(pairs):
            here = rows_of(g)
            prob = prob_ref[h, g]
            values = jnp.concatenate(
                [prior_value_ref[g * PAIR :, ch], v_ref[: (g + 1) * PAIR, ch]], axis=0
            )
            grad_probs = dot(grad[here], values, ((1,), (1,)))
            row_dot = jnp.sum(prob * grad_probs, axis=-1, keepdims=True)
            grad_scores = prob * (grad_probs - row_dot)
            grad_low = grad_scores.astype(bf16)
            low_ref[h, g] = grad_low
            summed_scores = grad_scores if summed_scores is None else summed_scores + grad_scores
        lower = pltpu.roll(summed_scores[SEG:], WINDOW - SEG, 1)
        lines.append(diagonal_sums(summed_scores[:SEG] + lower))
    line = jnp.concatenate(lines, axis=0)
    col = lax.broadcasted_iota(jnp.int32, line.shape, 1)
    wrapped = jnp.sum(jnp.where(col > REL, line, 0.0), axis=1, keepdims=True)
    line = jnp.where(col == 0, line + wrapped, line)
    table_ref[...] = jnp.broadcast_to(line[:, :REL][None], table_ref.shape)


def back_kernel(q_ref, weight_ref, grad_ref, low_ref, back_ref):
    rows, width = q_ref.shape
    heads, pairs = width // HEAD_DIM, rows // PAIR
    scale = 1.0 / math.sqrt(HEAD_DIM)
    for h in range(heads):
        ch = head_of(h)
        key_back = []
        value_back = []
        for g in range(pairs):
            here = rows_of(g)
            split = PRIOR - g * PAIR
            key_back.append(dot(low_ref[h, g, :, :split], q_ref[here, ch], ((0,), (0,))))
            value_back.append(dot(weight_ref[h, g, :, :split], grad_ref[here, ch], ((0,), (0,))))
        for parts, back_at, factor in ((key_back, 0, scale), (value_back, PRIOR, 1.0)):
            for g in range(pairs):
                total = sum(
                    (parts[a][(g - a) * PAIR : (g - a + 1) * PAIR] for a in range(1, g + 1)),
                    parts[0][rows_of(g)],
                )
                at = back_at + g * PAIR
                back_ref[at : at + PAIR, ch] = (total * factor).astype(bf16)


def late_kernel(q_ref, k_ref, prior_key_ref, weight_ref, grad_ref, low_ref, dq_ref, dk_ref, dv_ref):
    rows, width = q_ref.shape
    heads, pairs = width // HEAD_DIM, rows // PAIR
    scale = 1.0 / math.sqrt(HEAD_DIM)
    for h in range(heads):
        ch = head_of(h)
        key_own = []
        value_own = []
        for g in range(pairs):
            here = rows_of(g)
            split = PRIOR - g * PAIR
            low = low_ref[h, g]
            keys = jnp.concatenate(
                [prior_key_ref[g * PAIR : PRIOR, ch], k_ref[: (g + 1) * PAIR, ch]], axis=0
            )
            dq_ref[here, ch] = (dot(low, keys, ((1,), (0,))) * scale).astype(bf16)
            key_own.append(dot(low[:, split:], q_ref[here, ch], ((0,), (0,))))
            value_own.append(dot(weight_ref[h, g, :, split:], grad_ref[here, ch], ((0,), (0,))))
        for parts, own_ref, factor in ((key_own, dk_ref, scale), (value_own, dv_ref, 1.0)):
            for g in range(pairs):
                total = sum(
                    (parts[a][rows_of(g)] for a in range(g + 1, pairs)), parts[g][rows_of(g)]
                )
                own_ref[rows_of(g), ch] = total * factor


def final_kernel(dk_ref, dv_ref, back_ref, all_ref, turn_ref, key_ref, value_ref, table_ref):
    rows = dk_ref.shape[0]
    heads = table_ref.shape[0]
    key_ref[...] = (dk_ref[...] + back_ref[:rows].astype(f32)).astype(bf16)
    value_ref[...] = (dv_ref[...] + back_ref[rows:].astype(f32)).astype(bf16)
    pieces = jnp.concatenate(parts_of(jnp.sum(all_ref[...], axis=0), 3), axis=0)
    lines = dot(pieces, turn_ref[...], ((1,), (0,)))
    table_ref[...] = lines[2 * heads :] + lines[heads : 2 * heads] + lines[:heads]


def relay_kernel(all_ref, out_ref):
    out_ref[...] = jnp.broadcast_to(jnp.sum(all_ref[...], axis=0)[None], out_ref.shape)


def near(array):
    return pltpu.with_memory_space_constraint(array, pltpu.VMEM)


def far(array):
    return pltpu.with_memory_space_constraint(array, pltpu.HBM)


def call(kernel, outs, *arrays, scalars=0):
    many = isinstance(outs, tuple)
    return pl.pallas_call(
        kernel,
        out_shape=outs,
        in_specs=[SMEM] * scalars + [VMEM] * (len(arrays) - scalars),
        out_specs=(VMEM,) * len(outs) if many else VMEM,
        compiler_params=pltpu.CompilerParams(vmem_limit_bytes=ROOM),
    )(*arrays[:scalars], *(near(a) for a in arrays[scalars:]))


def on_device(queries, key_vectors, value_vectors, cotangent, out_gain, rel_table):
    shape = queries.shape
    rows, width = shape[1], shape[2]
    heads, pairs = width // HEAD_DIM, rows // PAIR
    q, k, v, cot = (a.reshape(rows, width) for a in (queries, key_vectors, value_vectors, cotangent))
    gain = out_gain.reshape(1, width)
    members = lax.axis_size("tp")
    tiles = (heads, pairs, PAIR, WINDOW)
    prior_keys = passed_along(k, SP, 1)
    prior_values = passed_along(v, SP, 1)
    first = (lax.axis_index(SP) == 0).astype(jnp.int32).reshape(1)
    own_block = kept((rows, width), bf16)
    q, k, v, own, bias, scaled, turn = pl.pallas_call(
        early_kernel,
        out_shape=(own_block,) * 3
        + (kept(tiles, f32), kept(tiles, f32), kept((rows, width), f32), kept((REL, REL), bf16)),
        in_specs=[SMEM, VMEM, VMEM] + [HBM] * 4,
        out_specs=(VMEM,) * 7,
        scratch_shapes=[pltpu.VMEM((rows, width), bf16), pltpu.SemaphoreType.DMA((4,))],
        compiler_params=pltpu.CompilerParams(vmem_limit_bytes=ROOM),
    )(first, near(rel_table), near(gain), *(far(a) for a in (q, k, cot, v)))
    prob, weight = call(
        weights_kernel, (kept(tiles, f32), kept(tiles, bf16)), q, prior_keys, own, bias
    )
    att, stat = call(
        forward_kernel,
        (kept((rows, width), f32), kept((members, 4, rows // 2), f32)),
        *(weight, v, prior_values, scaled),
    )
    stat = sent_to_all(stat, "tp", [ahead(list(range(members)), LEADER[2])])
    grad, low, table = call(
        functools.partial(middle_kernel, full_width=width * members),
        (
            kept((rows, width), bf16),
            kept(tiles, bf16),
            kept((12, heads, REL), f32),
        ),
        *(v, prior_values, scaled, prob, att, stat),
    )
    order = [ahead([z * 8 + y for z in range(12)], LEADER[0]) for y in range(8)]
    table = sent_to_all(table, SP, order)
    table = call(relay_kernel, kept((8, heads, REL), f32), table)
    order = [ahead([z * 8 + y for y in range(8)], LEADER[1]) for z in range(12)]
    table = sent_to_all(table, SP, order)
    back = call(back_kernel, kept((2 * rows, width), bf16), q, weight, grad, low)
    back = passed_along(back, SP, -1)
    dq, dk, dv = call(
        late_kernel,
        (out((rows, width), bf16), kept((rows, width), f32), kept((rows, width), f32)),
        *(q, k, prior_keys, weight, grad, low),
    )
    grad_keys, grad_values, grad_table = call(
        final_kernel,
        (out((rows, width), bf16), out((rows, width), bf16), out((heads, REL), f32)),
        *(dk, dv, back, table, turn),
    )
    return (dq.reshape(shape), grad_keys.reshape(shape), grad_values.reshape(shape), grad_table)


def solution(mesh):
    placed = (
        P(None, SP, "tp"),
        P(None, SP, "tp"),
        P(None, SP, "tp"),
        P(None, SP, "tp"),
        P("tp"),
        P("tp", None),
    )
    return jax.shard_map(
        on_device,
        mesh=mesh,
        in_specs=placed,
        out_specs=(P(None, SP, "tp"), P(None, SP, "tp"), P(None, SP, "tp"), P("tp", None)),
        check_vma=False,
    )
```

```python
import functools
import math

import jax
import jax.numpy as jnp
from jax import lax
from jax.experimental import pallas as pl
from jax.experimental.pallas import tpu as pltpu
from jax.sharding import PartitionSpec as P


HEAD_DIM = 128
SEG = 64
LEFT = 4
REL = 320
SP = "sp"
LEADER = (8, 4, 5)

PAIR = 2 * SEG
PRIOR = LEFT * SEG
WINDOW = PRIOR + PAIR
ROOM = 12 * 1024 * 1024
epsilon = 1e-06
masked_value = -1e30
f32 = jnp.float32
bf16 = jnp.bfloat16
kept = pltpu.VMEM
out = jax.ShapeDtypeStruct
VMEM = pl.BlockSpec(memory_space=pltpu.VMEM)
HBM = pl.BlockSpec(memory_space=pltpu.HBM)
SMEM = pl.BlockSpec(memory_space=pltpu.SMEM)


def dot(left, right, dims):
    return lax.dot_general(left, right, (dims, ((), ())), preferred_element_type=f32)


def parts_of(array, count):
    found = []
    for _ in range(count):
        found.append(array.astype(bf16))
        array = array - found[-1].astype(f32)
    return found


def passed_along(block, axis, distance):
    devices = range(lax.axis_size(axis))
    route = [(i - distance, i) for i in devices if i - distance in devices]
    return lax.ppermute(block, axis, route)


def ahead(group, leader):
    return [group[leader]] + group[:leader] + group[leader + 1 :]


def sent_to_all(copies, axis, order):
    return lax.all_to_all(
        copies, axis, split_axis=0, concat_axis=0, tiled=True, axis_index_groups=order
    )


def mirror(rows, cols):
    row_id = lax.broadcasted_iota(jnp.int32, (rows, cols), 0)
    col_id = lax.broadcasted_iota(jnp.int32, (rows, cols), 1)
    return row_id + col_id == REL - 1


def diagonal_sums(block):
    width = block.shape[1]
    folded = block[:8]
    for at in range(8, block.shape[0], 8):
        folded = folded + pltpu.roll(block[at : at + 8], width - at, 1)
    row = lax.broadcasted_iota(jnp.int32, folded.shape, 0)
    for step in (1, 2, 4):
        folded = jnp.where((row & step) != 0, pltpu.roll(folded, width - step, 1), folded)
    return jnp.sum(folded, axis=0, keepdims=True)


def head_of(h):
    return slice(h * HEAD_DIM, (h + 1) * HEAD_DIM)


def rows_of(g):
    return slice(g * PAIR, (g + 1) * PAIR)


def early_kernel(
    first_ref,
    rel_ref,
    gain_ref,
    q_hbm,
    k_hbm,
    cot_hbm,
    v_hbm,
    q_ref,
    k_ref,
    v_ref,
    own_ref,
    bias_ref,
    scaled_ref,
    turn_ref,
    cot_ref,
    sems,
):
    rows, width = q_ref.shape
    heads, pairs = width // HEAD_DIM, rows // PAIR
    scale = 1.0 / math.sqrt(HEAD_DIM)
    moves = ((q_hbm, q_ref), (k_hbm, k_ref), (cot_hbm, cot_ref), (v_hbm, v_ref))
    copies = [pltpu.make_async_copy(a, b, sems.at[i]) for i, (a, b) in enumerate(moves)]
    for copy in copies:
        copy.start()
    turn_ref[...] = mirror(REL, REL).astype(bf16)
    turned = dot(rel_ref[...], mirror(REL, WINDOW).astype(bf16), ((1,), (0,)))
    row = lax.broadcasted_iota(jnp.int32, (PAIR, WINDOW), 0)
    col = lax.broadcasted_iota(jnp.int32, (PAIR, WINDOW), 1)
    base = jnp.where(row >= SEG, SEG, 0)
    in_band = (col >= base) & (col < base + PRIOR + SEG)
    first = first_ref[0] == 1
    for h in range(heads):
        line = turned[h : h + 1]
        slid = pltpu.roll(jnp.broadcast_to(line, (PAIR, WINDOW)), 0, 1, stride=1, stride_axis=0)
        tile = jnp.where(col < row, jnp.broadcast_to(line[:, :1], (PAIR, WINDOW)), slid)
        tile = jnp.where(in_band, tile, masked_value)
        for g in range(pairs):
            split = PRIOR - g * PAIR
            prior = tile[:, :split]
            bias_ref[h, g, :, :split] = jnp.where(first, masked_value, prior)
            own_ref[h, g, :, split:] = tile[:, split:]
    copies[0].wait()
    copies[1].wait()
    for h in range(heads):
        for g in range(pairs):
            split = PRIOR - g * PAIR
            own = dot(q_ref[rows_of(g), head_of(h)], k_ref[: (g + 1) * PAIR, head_of(h)], ((1,), (1,)))
            own_ref[h, g, :, split:] += own * scale
    copies[2].wait()
    scaled_ref[...] = cot_ref[...].astype(f32) * gain_ref[...].astype(f32)
    copies[3].wait()


def weights_kernel(q_ref, prior_key_ref, own_ref, bias_ref, prob_ref, weight_ref):
    heads, pairs = prob_ref.shape[:2]
    scale = 1.0 / math.sqrt(HEAD_DIM)
    for h in range(heads):
        for g in range(pairs):
            split = PRIOR - g * PAIR
            keys = prior_key_ref[g * PAIR : PRIOR, head_of(h)]
            scores = dot(q_ref[rows_of(g), head_of(h)], keys, ((1,), (1,)))
            scores = scores * scale + bias_ref[h, g, :, :split]
            scores = jnp.concatenate([scores, own_ref[h, g, :, split:]], axis=1)
            top = jnp.max(scores, axis=-1, keepdims=True)
            shifted = jnp.exp(scores - top)
            prob = shifted * (1.0 / jnp.sum(shifted, axis=-1, keepdims=True))
            prob_ref[h, g] = prob
            weight_ref[h, g] = prob.astype(bf16)


def forward_kernel(weight_ref, v_ref, prior_value_ref, scaled_ref, att_ref, stat_ref):
    rows, width = v_ref.shape
    heads, pairs = width // HEAD_DIM, rows // PAIR
    squares = None
    products = None
    for h in range(heads):
        ch = head_of(h)
        outs = []
        for g in range(pairs):
            values = jnp.concatenate(
                [prior_value_ref[g * PAIR :, ch], v_ref[: (g + 1) * PAIR, ch]], axis=0
            )
            outs.append(dot(weight_ref[h, g], values, ((1,), (0,))))
        attended = jnp.concatenate(outs, axis=0)
        att_ref[:, ch] = attended
        square = attended * attended
        product = attended * scaled_ref[:, ch]
        squares = square if squares is None else squares + square
        products = product if products is None else products + product
    lines = []
    ones = jnp.ones((8, 2 * HEAD_DIM), bf16)
    for total in (squares, products):
        lines.append(dot(ones, jnp.concatenate(parts_of(total, 2), axis=1), ((1,), (1,)))[:1])
    half = rows // 2
    message = jnp.concatenate([x[:, at : at + half] for x in lines for at in (0, half)], axis=0)
    for d in range(stat_ref.shape[0]):
        stat_ref[d] = message


def middle_kernel(
    v_ref,
    prior_value_ref,
    scaled_ref,
    prob_ref,
    att_ref,
    stat_ref,
    grad_ref,
    low_ref,
    table_ref,
    *,
    full_width,
):
    rows, width = v_ref.shape
    heads, pairs = width // HEAD_DIM, rows // PAIR
    summed = stat_ref[0]
    for d in range(1, stat_ref.shape[0]):
        summed = summed + stat_ref[d]
    inv_line = lax.rsqrt(summed[:2] * (1.0 / full_width) + epsilon)
    pull_line = inv_line**3 * (summed[2:] * (1.0 / full_width))
    pieces = jnp.concatenate(parts_of(jnp.concatenate([inv_line, pull_line], axis=0), 3), axis=0)
    pick = lax.broadcasted_iota(jnp.int32, (12, 4 * HEAD_DIM), 1) // HEAD_DIM
    pick = (pick == lax.broadcasted_iota(jnp.int32, (12, 4 * HEAD_DIM), 0) % 4).astype(bf16)
    spread = dot(pieces, pick, ((0,), (0,)))
    inv_rms = jnp.concatenate([spread[:, :128], spread[:, 128:256]], axis=0)
    pull = jnp.concatenate([spread[:, 256:384], spread[:, 384:]], axis=0)
    lines = []
    for h in range(heads):
        ch = head_of(h)
        grad = (inv_rms * scaled_ref[:, ch] - att_ref[:, ch] * pull).astype(bf16)
        grad_ref[:, ch] = grad
        summed_scores = None
        for g in range(pairs):
            here = rows_of(g)
            prob = prob_ref[h, g]
            values = jnp.concatenate(
                [prior_value_ref[g * PAIR :, ch], v_ref[: (g + 1) * PAIR, ch]], axis=0
            )
            grad_probs = dot(grad[here], values, ((1,), (1,)))
            row_dot = jnp.sum(prob * grad_probs, axis=-1, keepdims=True)
            grad_scores = prob * (grad_probs - row_dot)
            grad_low = grad_scores.astype(bf16)
            low_ref[h, g] = grad_low
            summed_scores = grad_scores if summed_scores is None else summed_scores + grad_scores
        lower = pltpu.roll(summed_scores[SEG:], WINDOW - SEG, 1)
        lines.append(diagonal_sums(summed_scores[:SEG] + lower))
    line = jnp.concatenate(lines, axis=0)
    col = lax.broadcasted_iota(jnp.int32, line.shape, 1)
    wrapped = jnp.sum(jnp.where(col > REL, line, 0.0), axis=1, keepdims=True)
    line = jnp.where(col == 0, line + wrapped, line)
    table_ref[...] = jnp.broadcast_to(line[:, :REL][None], table_ref.shape)


def back_kernel(q_ref, weight_ref, grad_ref, low_ref, back_ref):
    rows, width = q_ref.shape
    heads, pairs = width // HEAD_DIM, rows // PAIR
    scale = 1.0 / math.sqrt(HEAD_DIM)
    for h in range(heads):
        ch = head_of(h)
        key_back = []
        value_back = []
        for g in range(pairs):
            here = rows_of(g)
            split = PRIOR - g * PAIR
            key_back.append(dot(low_ref[h, g, :, :split], q_ref[here, ch], ((0,), (0,))))
            value_back.append(dot(weight_ref[h, g, :, :split], grad_ref[here, ch], ((0,), (0,))))
        for parts, back_at, factor in ((key_back, 0, scale), (value_back, PRIOR, 1.0)):
            for g in range(pairs):
                total = sum(
                    (parts[a][(g - a) * PAIR : (g - a + 1) * PAIR] for a in range(1, g + 1)),
                    parts[0][rows_of(g)],
                )
                at = back_at + g * PAIR
                back_ref[at : at + PAIR, ch] = (total * factor).astype(bf16)


def late_kernel(q_ref, k_ref, prior_key_ref, weight_ref, grad_ref, low_ref, dq_ref, dk_ref, dv_ref):
    rows, width = q_ref.shape
    heads, pairs = width // HEAD_DIM, rows // PAIR
    scale = 1.0 / math.sqrt(HEAD_DIM)
    for h in range(heads):
        ch = head_of(h)
        key_own = []
        value_own = []
        for g in range(pairs):
            here = rows_of(g)
            split = PRIOR - g * PAIR
            low = low_ref[h, g]
            keys = jnp.concatenate(
                [prior_key_ref[g * PAIR : PRIOR, ch], k_ref[: (g + 1) * PAIR, ch]], axis=0
            )
            dq_ref[here, ch] = (dot(low, keys, ((1,), (0,))) * scale).astype(bf16)
            key_own.append(dot(low[:, split:], q_ref[here, ch], ((0,), (0,))))
            value_own.append(dot(weight_ref[h, g, :, split:], grad_ref[here, ch], ((0,), (0,))))
        for parts, own_ref, factor in ((key_own, dk_ref, scale), (value_own, dv_ref, 1.0)):
            for g in range(pairs):
                total = sum(
                    (parts[a][rows_of(g)] for a in range(g + 1, pairs)), parts[g][rows_of(g)]
                )
                own_ref[rows_of(g), ch] = total * factor


def final_kernel(dk_ref, dv_ref, back_ref, all_ref, turn_ref, key_ref, value_ref, table_ref):
    rows = dk_ref.shape[0]
    heads = table_ref.shape[0]
    key_ref[...] = (dk_ref[...] + back_ref[:rows].astype(f32)).astype(bf16)
    value_ref[...] = (dv_ref[...] + back_ref[rows:].astype(f32)).astype(bf16)
    pieces = jnp.concatenate(parts_of(jnp.sum(all_ref[...], axis=0), 3), axis=0)
    lines = dot(pieces, turn_ref[...], ((1,), (0,)))
    table_ref[...] = lines[2 * heads :] + lines[heads : 2 * heads] + lines[:heads]


def relay_kernel(all_ref, out_ref):
    out_ref[...] = jnp.broadcast_to(jnp.sum(all_ref[...], axis=0)[None], out_ref.shape)


def near(array):
    return pltpu.with_memory_space_constraint(array, pltpu.VMEM)


def far(array):
    return pltpu.with_memory_space_constraint(array, pltpu.HBM)


def call(kernel, outs, *arrays, scalars=0):
    many = isinstance(outs, tuple)
    return pl.pallas_call(
        kernel,
        out_shape=outs,
        in_specs=[SMEM] * scalars + [VMEM] * (len(arrays) - scalars),
        out_specs=(VMEM,) * len(outs) if many else VMEM,
        compiler_params=pltpu.CompilerParams(vmem_limit_bytes=ROOM),
    )(*arrays[:scalars], *(near(a) for a in arrays[scalars:]))


def on_device(queries, key_vectors, value_vectors, cotangent, out_gain, rel_table):
    shape = queries.shape
    rows, width = shape[1], shape[2]
    heads, pairs = width // HEAD_DIM, rows // PAIR
    q, k, v, cot = (a.reshape(rows, width) for a in (queries, key_vectors, value_vectors, cotangent))
    gain = out_gain.reshape(1, width)
    members = lax.axis_size("tp")
    tiles = (heads, pairs, PAIR, WINDOW)
    prior_keys = passed_along(k, SP, 1)
    prior_values = passed_along(v, SP, 1)
    first = (lax.axis_index(SP) == 0).astype(jnp.int32).reshape(1)
    own_block = kept((rows, width), bf16)
    q, k, v, own, bias, scaled, turn = pl.pallas_call(
        early_kernel,
        out_shape=(own_block,) * 3
        + (kept(tiles, f32), kept(tiles, f32), kept((rows, width), f32), kept((REL, REL), bf16)),
        in_specs=[SMEM, VMEM, VMEM] + [HBM] * 4,
        out_specs=(VMEM,) * 7,
        scratch_shapes=[pltpu.VMEM((rows, width), bf16), pltpu.SemaphoreType.DMA((4,))],
        compiler_params=pltpu.CompilerParams(vmem_limit_bytes=ROOM),
    )(first, near(rel_table), near(gain), *(far(a) for a in (q, k, cot, v)))
    prob, weight = call(
        weights_kernel, (kept(tiles, f32), kept(tiles, bf16)), q, prior_keys, own, bias
    )
    att, stat = call(
        forward_kernel,
        (kept((rows, width), f32), kept((members, 4, rows // 2), f32)),
        *(weight, v, prior_values, scaled),
    )
    stat = sent_to_all(stat, "tp", [ahead(list(range(members)), LEADER[2])])
    grad, low, table = call(
        functools.partial(middle_kernel, full_width=width * members),
        (
            kept((rows, width), bf16),
            kept(tiles, bf16),
            kept((12, heads, REL), f32),
        ),
        *(v, prior_values, scaled, prob, att, stat),
    )
    order = [ahead([z * 8 + y for z in range(12)], LEADER[0]) for y in range(8)]
    table = sent_to_all(table, SP, order)
    table = call(relay_kernel, kept((8, heads, REL), f32), table)
    order = [ahead([z * 8 + y for y in range(8)], LEADER[1]) for z in range(12)]
    table = sent_to_all(table, SP, order)
    back = call(back_kernel, kept((2 * rows, width), bf16), q, weight, grad, low)
    back = passed_along(back, SP, -1)
    dq, dk, dv = call(
        late_kernel,
        (out((rows, width), bf16), kept((rows, width), f32), kept((rows, width), f32)),
        *(q, k, prior_keys, weight, grad, low),
    )
    grad_keys, grad_values, grad_table = call(
        final_kernel,
        (out((rows, width), bf16), out((rows, width), bf16), out((heads, REL), f32)),
        *(dk, dv, back, table, turn),
    )
    return (dq.reshape(shape), grad_keys.reshape(shape), grad_values.reshape(shape), grad_table)


def solution(mesh):
    placed = (
        P(None, SP, "tp"),
        P(None, SP, "tp"),
        P(None, SP, "tp"),
        P(None, SP, "tp"),
        P("tp"),
        P("tp", None),
    )
    return jax.shard_map(
        on_device,
        mesh=mesh,
        in_specs=placed,
        out_specs=(P(None, SP, "tp"), P(None, SP, "tp"), P(None, SP, "tp"), P("tp", None)),
        check_vma=False,
    )
```

```python
import functools
import math

import jax
import jax.numpy as jnp
from jax import lax
from jax.experimental import pallas as pl
from jax.experimental.pallas import tpu as pltpu
from jax.sharding import PartitionSpec as P


HEAD_DIM = 128
SEG = 64
LEFT = 4
REL = 320
SP = "sp"
LEADER = (8, 4, 5)

PAIR = 2 * SEG
PRIOR = LEFT * SEG
WINDOW = PRIOR + PAIR
ROOM = 12 * 1024 * 1024
epsilon = 1e-06
masked_value = -1e30
f32 = jnp.float32
bf16 = jnp.bfloat16
kept = pltpu.VMEM
out = jax.ShapeDtypeStruct
VMEM = pl.BlockSpec(memory_space=pltpu.VMEM)
HBM = pl.BlockSpec(memory_space=pltpu.HBM)
SMEM = pl.BlockSpec(memory_space=pltpu.SMEM)


def dot(left, right, dims):
    return lax.dot_general(left, right, (dims, ((), ())), preferred_element_type=f32)


def parts_of(array, count):
    found = []
    for _ in range(count):
        found.append(array.astype(bf16))
        array = array - found[-1].astype(f32)
    return found


def passed_along(block, axis, distance):
    devices = range(lax.axis_size(axis))
    route = [(i - distance, i) for i in devices if i - distance in devices]
    return lax.ppermute(block, axis, route)


def ahead(group, leader):
    return [group[leader]] + group[:leader] + group[leader + 1 :]


def sent_to_all(copies, axis, order):
    return lax.all_to_all(
        copies, axis, split_axis=0, concat_axis=0, tiled=True, axis_index_groups=order
    )


def mirror(rows, cols):
    row_id = lax.broadcasted_iota(jnp.int32, (rows, cols), 0)
    col_id = lax.broadcasted_iota(jnp.int32, (rows, cols), 1)
    return row_id + col_id == REL - 1


def diagonal_sums(block):
    width = block.shape[1]
    folded = block[:8]
    for at in range(8, block.shape[0], 8):
        folded = folded + pltpu.roll(block[at : at + 8], width - at, 1)
    row = lax.broadcasted_iota(jnp.int32, folded.shape, 0)
    for step in (1, 2, 4):
        folded = jnp.where((row & step) != 0, pltpu.roll(folded, width - step, 1), folded)
    return jnp.sum(folded, axis=0, keepdims=True)


def head_of(h):
    return slice(h * HEAD_DIM, (h + 1) * HEAD_DIM)


def rows_of(g):
    return slice(g * PAIR, (g + 1) * PAIR)


def early_kernel(
    first_ref,
    rel_ref,
    gain_ref,
    q_hbm,
    k_hbm,
    cot_hbm,
    v_hbm,
    q_ref,
    k_ref,
    v_ref,
    own_ref,
    bias_ref,
    scaled_ref,
    turn_ref,
    cot_ref,
    sems,
):
    rows, width = q_ref.shape
    heads, pairs = width // HEAD_DIM, rows // PAIR
    scale = 1.0 / math.sqrt(HEAD_DIM)
    moves = ((q_hbm, q_ref), (k_hbm, k_ref), (cot_hbm, cot_ref), (v_hbm, v_ref))
    copies = [pltpu.make_async_copy(a, b, sems.at[i]) for i, (a, b) in enumerate(moves)]
    for copy in copies:
        copy.start()
    turn_ref[...] = mirror(REL, REL).astype(bf16)
    turned = dot(rel_ref[...], mirror(REL, WINDOW).astype(bf16), ((1,), (0,)))
    row = lax.broadcasted_iota(jnp.int32, (PAIR, WINDOW), 0)
    col = lax.broadcasted_iota(jnp.int32, (PAIR, WINDOW), 1)
    base = jnp.where(row >= SEG, SEG, 0)
    in_band = (col >= base) & (col < base + PRIOR + SEG)
    first = first_ref[0] == 1
    for h in range(heads):
        line = turned[h : h + 1]
        slid = pltpu.roll(jnp.broadcast_to(line, (PAIR, WINDOW)), 0, 1, stride=1, stride_axis=0)
        tile = jnp.where(col < row, jnp.broadcast_to(line[:, :1], (PAIR, WINDOW)), slid)
        tile = jnp.where(in_band, tile, masked_value)
        for g in range(pairs):
            split = PRIOR - g * PAIR
            prior = tile[:, :split]
            bias_ref[h, g, :, :split] = jnp.where(first, masked_value, prior)
            own_ref[h, g, :, split:] = tile[:, split:]
    copies[0].wait()
    copies[1].wait()
    for h in range(heads):
        for g in range(pairs):
            split = PRIOR - g * PAIR
            own = dot(q_ref[rows_of(g), head_of(h)], k_ref[: (g + 1) * PAIR, head_of(h)], ((1,), (1,)))
            own_ref[h, g, :, split:] += own * scale
    copies[2].wait()
    scaled_ref[...] = cot_ref[...].astype(f32) * gain_ref[...].astype(f32)
    copies[3].wait()


def weights_kernel(q_ref, prior_key_ref, own_ref, bias_ref, prob_ref, weight_ref):
    heads, pairs = prob_ref.shape[:2]
    scale = 1.0 / math.sqrt(HEAD_DIM)
    for h in range(heads):
        for g in range(pairs):
            split = PRIOR - g * PAIR
            keys = prior_key_ref[g * PAIR : PRIOR, head_of(h)]
            scores = dot(q_ref[rows_of(g), head_of(h)], keys, ((1,), (1,)))
            scores = scores * scale + bias_ref[h, g, :, :split]
            scores = jnp.concatenate([scores, own_ref[h, g, :, split:]], axis=1)
            top = jnp.max(scores, axis=-1, keepdims=True)
            shifted = jnp.exp(scores - top)
            prob = shifted * (1.0 / jnp.sum(shifted, axis=-1, keepdims=True))
            prob_ref[h, g] = prob
            weight_ref[h, g] = prob.astype(bf16)


def forward_kernel(weight_ref, v_ref, prior_value_ref, scaled_ref, att_ref, stat_ref):
    rows, width = v_ref.shape
    heads, pairs = width // HEAD_DIM, rows // PAIR
    squares = None
    products = None
    for h in range(heads):
        ch = head_of(h)
        outs = []
        for g in range(pairs):
            values = jnp.concatenate(
                [prior_value_ref[g * PAIR :, ch], v_ref[: (g + 1) * PAIR, ch]], axis=0
            )
            outs.append(dot(weight_ref[h, g], values, ((1,), (0,))))
        attended = jnp.concatenate(outs, axis=0)
        att_ref[:, ch] = attended
        square = attended * attended
        product = attended * scaled_ref[:, ch]
        squares = square if squares is None else squares + square
        products = product if products is None else products + product
    lines = []
    ones = jnp.ones((8, 2 * HEAD_DIM), bf16)
    for total in (squares, products):
        lines.append(dot(ones, jnp.concatenate(parts_of(total, 2), axis=1), ((1,), (1,)))[:1])
    half = rows // 2
    message = jnp.concatenate([x[:, at : at + half] for x in lines for at in (0, half)], axis=0)
    for d in range(stat_ref.shape[0]):
        stat_ref[d] = message


def middle_kernel(
    v_ref,
    prior_value_ref,
    scaled_ref,
    prob_ref,
    att_ref,
    stat_ref,
    grad_ref,
    low_ref,
    table_ref,
    *,
    full_width,
):
    rows, width = v_ref.shape
    heads, pairs = width // HEAD_DIM, rows // PAIR
    summed = stat_ref[0]
    for d in range(1, stat_ref.shape[0]):
        summed = summed + stat_ref[d]
    inv_line = lax.rsqrt(summed[:2] * (1.0 / full_width) + epsilon)
    pull_line = inv_line**3 * (summed[2:] * (1.0 / full_width))
    pieces = jnp.concatenate(parts_of(jnp.concatenate([inv_line, pull_line], axis=0), 3), axis=0)
    pick = lax.broadcasted_iota(jnp.int32, (12, 4 * HEAD_DIM), 1) // HEAD_DIM
    pick = (pick == lax.broadcasted_iota(jnp.int32, (12, 4 * HEAD_DIM), 0) % 4).astype(bf16)
    spread = dot(pieces, pick, ((0,), (0,)))
    inv_rms = jnp.concatenate([spread[:, :128], spread[:, 128:256]], axis=0)
    pull = jnp.concatenate([spread[:, 256:384], spread[:, 384:]], axis=0)
    lines = []
    for h in range(heads):
        ch = head_of(h)
        grad = (inv_rms * scaled_ref[:, ch] - att_ref[:, ch] * pull).astype(bf16)
        grad_ref[:, ch] = grad
        summed_scores = None
        for g in range(pairs):
            here = rows_of(g)
            prob = prob_ref[h, g]
            values = jnp.concatenate(
                [prior_value_ref[g * PAIR :, ch], v_ref[: (g + 1) * PAIR, ch]], axis=0
            )
            grad_probs = dot(grad[here], values, ((1,), (1,)))
            row_dot = jnp.sum(prob * grad_probs, axis=-1, keepdims=True)
            grad_scores = prob * (grad_probs - row_dot)
            grad_low = grad_scores.astype(bf16)
            low_ref[h, g] = grad_low
            summed_scores = grad_scores if summed_scores is None else summed_scores + grad_scores
        lower = pltpu.roll(summed_scores[SEG:], WINDOW - SEG, 1)
        lines.append(diagonal_sums(summed_scores[:SEG] + lower))
    line = jnp.concatenate(lines, axis=0)
    col = lax.broadcasted_iota(jnp.int32, line.shape, 1)
    wrapped = jnp.sum(jnp.where(col > REL, line, 0.0), axis=1, keepdims=True)
    line = jnp.where(col == 0, line + wrapped, line)
    table_ref[...] = jnp.broadcast_to(line[:, :REL][None], table_ref.shape)


def back_kernel(q_ref, weight_ref, grad_ref, low_ref, back_ref):
    rows, width = q_ref.shape
    heads, pairs = width // HEAD_DIM, rows // PAIR
    scale = 1.0 / math.sqrt(HEAD_DIM)
    for h in range(heads):
        ch = head_of(h)
        key_back = []
        value_back = []
        for g in range(pairs):
            here = rows_of(g)
            split = PRIOR - g * PAIR
            key_back.append(dot(low_ref[h, g, :, :split], q_ref[here, ch], ((0,), (0,))))
            value_back.append(dot(weight_ref[h, g, :, :split], grad_ref[here, ch], ((0,), (0,))))
        for parts, back_at, factor in ((key_back, 0, scale), (value_back, PRIOR, 1.0)):
            for g in range(pairs):
                total = sum(
                    (parts[a][(g - a) * PAIR : (g - a + 1) * PAIR] for a in range(1, g + 1)),
                    parts[0][rows_of(g)],
                )
                at = back_at + g * PAIR
                back_ref[at : at + PAIR, ch] = (total * factor).astype(bf16)


def late_kernel(q_ref, k_ref, prior_key_ref, weight_ref, grad_ref, low_ref, dq_ref, dk_ref, dv_ref):
    rows, width = q_ref.shape
    heads, pairs = width // HEAD_DIM, rows // PAIR
    scale = 1.0 / math.sqrt(HEAD_DIM)
    for h in range(heads):
        ch = head_of(h)
        key_own = []
        value_own = []
        for g in range(pairs):
            here = rows_of(g)
            split = PRIOR - g * PAIR
            low = low_ref[h, g]
            keys = jnp.concatenate(
                [prior_key_ref[g * PAIR : PRIOR, ch], k_ref[: (g + 1) * PAIR, ch]], axis=0
            )
            dq_ref[here, ch] = (dot(low, keys, ((1,), (0,))) * scale).astype(bf16)
            key_own.append(dot(low[:, split:], q_ref[here, ch], ((0,), (0,))))
            value_own.append(dot(weight_ref[h, g, :, split:], grad_ref[here, ch], ((0,), (0,))))
        for parts, own_ref, factor in ((key_own, dk_ref, scale), (value_own, dv_ref, 1.0)):
            for g in range(pairs):
                total = sum(
                    (parts[a][rows_of(g)] for a in range(g + 1, pairs)), parts[g][rows_of(g)]
                )
                own_ref[rows_of(g), ch] = total * factor


def final_kernel(
    dk_ref,
    dv_ref,
    back_ref,
    all_ref,
    turn_ref,
    key_hbm,
    value_hbm,
    table_hbm,
    key_ref,
    value_ref,
    table_ref,
    sems,
):
    rows = dk_ref.shape[0]
    heads = table_ref.shape[0]
    moves = ((key_ref, key_hbm), (value_ref, value_hbm), (table_ref, table_hbm))
    copies = [pltpu.make_async_copy(a, b, sems.at[i]) for i, (a, b) in enumerate(moves)]
    key_ref[...] = (dk_ref[...] + back_ref[:rows].astype(f32)).astype(bf16)
    copies[0].start()
    value_ref[...] = (dv_ref[...] + back_ref[rows:].astype(f32)).astype(bf16)
    copies[1].start()
    pieces = jnp.concatenate(parts_of(jnp.sum(all_ref[...], axis=0), 3), axis=0)
    lines = dot(pieces, turn_ref[...], ((1,), (0,)))
    table_ref[...] = lines[2 * heads :] + lines[heads : 2 * heads] + lines[:heads]
    copies[2].start()
    for copy in copies:
        copy.wait()


def relay_kernel(all_ref, out_ref):
    out_ref[...] = jnp.broadcast_to(jnp.sum(all_ref[...], axis=0)[None], out_ref.shape)


def near(array):
    return pltpu.with_memory_space_constraint(array, pltpu.VMEM)


def far(array):
    return pltpu.with_memory_space_constraint(array, pltpu.HBM)


def call(kernel, outs, *arrays, scalars=0):
    many = isinstance(outs, tuple)
    return pl.pallas_call(
        kernel,
        out_shape=outs,
        in_specs=[SMEM] * scalars + [VMEM] * (len(arrays) - scalars),
        out_specs=(VMEM,) * len(outs) if many else VMEM,
        compiler_params=pltpu.CompilerParams(vmem_limit_bytes=ROOM),
    )(*arrays[:scalars], *(near(a) for a in arrays[scalars:]))


def on_device(queries, key_vectors, value_vectors, cotangent, out_gain, rel_table):
    shape = queries.shape
    rows, width = shape[1], shape[2]
    heads, pairs = width // HEAD_DIM, rows // PAIR
    q, k, v, cot = (a.reshape(rows, width) for a in (queries, key_vectors, value_vectors, cotangent))
    gain = out_gain.reshape(1, width)
    members = lax.axis_size("tp")
    tiles = (heads, pairs, PAIR, WINDOW)
    prior_keys = passed_along(k, SP, 1)
    prior_values = passed_along(v, SP, 1)
    first = (lax.axis_index(SP) == 0).astype(jnp.int32).reshape(1)
    own_block = kept((rows, width), bf16)
    q, k, v, own, bias, scaled, turn = pl.pallas_call(
        early_kernel,
        out_shape=(own_block,) * 3
        + (kept(tiles, f32), kept(tiles, f32), kept((rows, width), f32), kept((REL, REL), bf16)),
        in_specs=[SMEM, VMEM, VMEM] + [HBM] * 4,
        out_specs=(VMEM,) * 7,
        scratch_shapes=[pltpu.VMEM((rows, width), bf16), pltpu.SemaphoreType.DMA((4,))],
        compiler_params=pltpu.CompilerParams(vmem_limit_bytes=ROOM),
    )(first, near(rel_table), near(gain), *(far(a) for a in (q, k, cot, v)))
    prob, weight = call(
        weights_kernel, (kept(tiles, f32), kept(tiles, bf16)), q, prior_keys, own, bias
    )
    att, stat = call(
        forward_kernel,
        (kept((rows, width), f32), kept((members, 4, rows // 2), f32)),
        *(weight, v, prior_values, scaled),
    )
    stat = sent_to_all(stat, "tp", [ahead(list(range(members)), LEADER[2])])
    grad, low, table = call(
        functools.partial(middle_kernel, full_width=width * members),
        (
            kept((rows, width), bf16),
            kept(tiles, bf16),
            kept((12, heads, REL), f32),
        ),
        *(v, prior_values, scaled, prob, att, stat),
    )
    order = [ahead([z * 8 + y for z in range(12)], LEADER[0]) for y in range(8)]
    table = sent_to_all(table, SP, order)
    table = call(relay_kernel, kept((8, heads, REL), f32), table)
    order = [ahead([z * 8 + y for y in range(8)], LEADER[1]) for z in range(12)]
    table = sent_to_all(table, SP, order)
    back = call(back_kernel, kept((2 * rows, width), bf16), q, weight, grad, low)
    back = passed_along(back, SP, -1)
    dq, dk, dv = call(
        late_kernel,
        (out((rows, width), bf16), kept((rows, width), f32), kept((rows, width), f32)),
        *(q, k, prior_keys, weight, grad, low),
    )
    grad_keys, grad_values, grad_table = pl.pallas_call(
        final_kernel,
        out_shape=(
            pltpu.HBM((rows, width), bf16),
            pltpu.HBM((rows, width), bf16),
            pltpu.HBM((heads, REL), f32),
        ),
        in_specs=[VMEM] * 5,
        out_specs=(HBM,) * 3,
        scratch_shapes=[
            pltpu.VMEM((rows, width), bf16),
            pltpu.VMEM((rows, width), bf16),
            pltpu.VMEM((heads, REL), f32),
            pltpu.SemaphoreType.DMA((3,)),
        ],
        compiler_params=pltpu.CompilerParams(vmem_limit_bytes=ROOM),
    )(*(near(a) for a in (dk, dv, back, table, turn)))
    return (dq.reshape(shape), grad_keys.reshape(shape), grad_values.reshape(shape), grad_table)


def solution(mesh):
    placed = (
        P(None, SP, "tp"),
        P(None, SP, "tp"),
        P(None, SP, "tp"),
        P(None, SP, "tp"),
        P("tp"),
        P("tp", None),
    )
    return jax.shard_map(
        on_device,
        mesh=mesh,
        in_specs=placed,
        out_specs=(P(None, SP, "tp"), P(None, SP, "tp"), P(None, SP, "tp"), P("tp", None)),
        check_vma=False,
    )
```
